256 devices in a mesh: grp: 2 (over y), sp: 16 (over z), fs: 4 (over x), tp: 2 (over core).
Axes of the slice: x: 4, y: 2, z: 16, core: 2. Of those that a mesh axis runs over, the one named last changes fastest.
The devices are a block of a 4x16x16 slice.
Arguments:
- tokens: bfloat16 [8, 2048, 2048], P(('grp', 'fs'), 'sp', 'tp'), parts along dimension 0, may hold values from -6 to 6
- norm_gain: float32 [2048], replicated, may hold values from 0.1 to 1.9
- w_z: bfloat16 [2048, 2048], P(('sp', 'fs'), 'tp'), may hold values from -0.125 to 0.125
- w_x: bfloat16 [2048, 2048], P(('sp', 'fs'), 'tp'), may hold values from -0.125 to 0.125
- w_b: bfloat16 [2048, 512], P(('sp', 'fs'), 'tp'), may hold values from -0.125 to 0.125
- w_c: bfloat16 [2048, 512], P(('sp', 'fs'), 'tp'), may hold values from -0.125 to 0.125
- w_dt: bfloat16 [2048, 32], P(None, 'tp'), may hold values from -0.125 to 0.125
- w_gate: bfloat16 [2048, 2, 32], P(None, None, 'tp'), may hold values from -0.125 to 0.125
- w_scb: bfloat16 [2048, 2048], P(('sp', 'fs'), 'tp'), may hold values from -0.125 to 0.125
- w_scc: bfloat16 [2048, 2048], P(('sp', 'fs'), 'tp'), may hold values from -0.125 to 0.125
- w_scx: bfloat16 [2048, 2048], P(('sp', 'fs'), 'tp'), may hold values from -0.125 to 0.125
- conv_x: float32 [4, 2048], P(None, 'tp'), may hold values from -3 to 3
- conv_b: float32 [4, 512], P(None, 'tp'), may hold values from -3 to 3
- conv_c: float32 [4, 512], P(None, 'tp'), may hold values from -3 to 3
- conv_sc: float32 [3, 2048], P(None, 'tp'), may hold values from -8 to 8
- dt_bias: float32 [32], P('tp'), may hold values from -1 to 1
- decay_log: float32 [32], P('tp'), as said below
- group_gain: float32 [2048], P('tp'), may hold values from 0.1 to 1.9
- span_shift: float32 [8, 32], P(('grp', 'fs'), 'sp'), parts along dimension 0, may hold values from -1.5 to 1.5
- w_out: bfloat16 [2048, 2048], P(('sp', 'fs'), 'tp'), may hold values from -0.125 to 0.125
Outputs:
- mixed: bfloat16 [8, 2048, 2048], P(('grp', 'fs'), ('sp', 'tp')), parts along dimension 0
The draws below stay inside these ranges and needn't reach their ends.
There are 2 independent parts, one for each index of `grp`. The reference program is written for one: setup_inputs(seed, part) draws one part's arguments, and reference() takes and returns one part's arrays. A program takes and returns all parts, laid end to end along the dimension named above; an argument that names none is the same for every part. Nothing has to cross between parts.
Inputs may be any that keep to these rules, and one draw needn't show every extreme that they name: `decay_log`: one value a head.
All inputs are finite; a program needn't handle non-finite values.
Results may differ from the reference program's by a relative error of at most 0.014.
Values may be sent and summed in bfloat16 or wider, within the bound.
No kernel may reach another device: no remote copies, remote signals or barrier semaphores. Data moves between devices by JAX's collectives and lax.ppermute only.
A program may use at most 128 MiB of HBM per device.

```python
import jax
import jax.numpy as jnp
from jax import lax

D = 2048
HEADS = 32
HEAD_DIM = 64
GROUPS = 8
STATE = 64
K_SSD = 4
K_SC = 3
BLOCK = 64
INNER = 2048
SHARE = 1024
SEQ = 2048
BATCH = 4
SPANS = 32


def draw_decay_log(key, part):
    order_key, slow_key, fast_key = jax.random.split(key, 3)
    order = jax.random.permutation(order_key, HEADS)
    fast = order < HEADS // 2
    slow_rate = jnp.exp(jax.random.uniform(slow_key, (HEADS,), jnp.float32, jnp.log(0.02), jnp.log(0.2))) / SEQ
    fast_rate = jnp.exp(jax.random.uniform(fast_key, (HEADS,), jnp.float32, jnp.log(0.015), jnp.log(0.04)))
    return jnp.log(jnp.where(fast, fast_rate, slow_rate)).astype(jnp.float32)


def levels(stream_key, extent, pieces, smallest, largest):
    gain = 1.0
    for position, blocks in pieces:
        draws = jax.random.uniform(jax.random.fold_in(jax.random.fold_in(stream_key, 6), position), (blocks,), jnp.float32, smallest / len(pieces), largest / len(pieces))
        gain = gain * jnp.repeat(jnp.exp(draws), extent[position] // blocks).reshape((-1,) + (1,) * (len(extent) - 1 - position))
    return gain


def bell_draw(stream_key, dims, spread, bound, shards=(), kind=jnp.bfloat16):
    entries = jax.random.normal(stream_key, dims, jnp.float32) * spread
    if len(shards) > 0:
        entries = levels(stream_key, dims, shards, -0.22, 0.18) * entries
    return jnp.clip(entries, min=-bound, max=bound).astype(kind)


def setup_inputs(seed: int = 0, part: int = 0) -> dict:
    arg_keys = jax.random.split(jax.random.key(seed), 21)
    own_keys = jax.random.split(jax.random.fold_in(arg_keys[20], part), 21)
    return {
        "tokens": bell_draw(own_keys[0], (BATCH, SEQ, D), 1.0, 6.0, ((0, 4), (1, 16), (2, 2))),
        "norm_gain": jnp.clip(1.0 + 0.18 * jax.random.normal(arg_keys[1], (D,), jnp.float32), 0.1, 1.9),
        "w_z": bell_draw(arg_keys[2], (D, INNER), D ** -0.5, 0.125, ((0, 64), (1, 2))),
        "w_x": bell_draw(arg_keys[3], (D, INNER), D ** -0.5, 0.125, ((0, 64), (1, 2))),
        "w_b": bell_draw(arg_keys[4], (D, GROUPS * STATE), D ** -0.5, 0.125, ((0, 64), (1, 2))),
        "w_c": bell_draw(arg_keys[5], (D, GROUPS * STATE), D ** -0.5, 0.125, ((0, 64), (1, 2))),
        "w_dt": bell_draw(arg_keys[6], (D, HEADS), D ** -0.5, 0.125, ((1, 2),)),
        "w_gate": bell_draw(arg_keys[7], (D, 2, HEADS), D ** -0.5, 0.125, ((2, 2),)),
        "w_scb": bell_draw(arg_keys[8], (D, INNER), D ** -0.5, 0.125, ((0, 64), (1, 2))),
        "w_scc": bell_draw(arg_keys[9], (D, INNER), D ** -0.5, 0.125, ((0, 64), (1, 2))),
        "w_scx": bell_draw(arg_keys[10], (D, INNER), D ** -0.5, 0.125, ((0, 64), (1, 2))),
        "conv_x": bell_draw(arg_keys[11], (K_SSD, INNER), 0.5, 3.0, ((1, 2),), jnp.float32),
        "conv_b": bell_draw(arg_keys[12], (K_SSD, GROUPS * STATE), 0.5, 3.0, ((1, 2),), jnp.float32),
        "conv_c": bell_draw(arg_keys[13], (K_SSD, GROUPS * STATE), 0.5, 3.0, ((1, 2),), jnp.float32),
        "conv_sc": bell_draw(arg_keys[14], (K_SC, INNER), 1.5, 8.0, ((1, 2),), jnp.float32),
        "dt_bias": jnp.clip(jax.random.uniform(arg_keys[15], (HEADS,), jnp.float32, -1.0, 1.0) * levels(arg_keys[15], (HEADS,), ((0, 2),), -0.4, 0.0), -1.0, 1.0),
        "decay_log": draw_decay_log(jax.random.fold_in(arg_keys[20], 71), part),
        "group_gain": jnp.clip(1.0 + 0.18 * jax.random.normal(arg_keys[17], (INNER,), jnp.float32), 0.1, 1.9),
        "span_shift": jnp.clip(jax.random.uniform(own_keys[18], (BATCH, SPANS), jnp.float32, -1.5, 1.5) * levels(own_keys[18], (BATCH, SPANS), ((0, 4), (1, 16)), -0.4, 0.0), -1.5, 1.5),
        "w_out": bell_draw(arg_keys[19], (D, INNER), INNER ** -0.5, 0.125, ((0, 64), (1, 2))),
    }


EPS = 1.0
HIGH = lax.Precision.HIGHEST

def causal_taps(padded, taps):
    width = taps.shape[0]
    length = padded.shape[1] - width + 1
    result = padded[:, 0:length] * taps[0]
    for step in range(1, width):
        result = result + padded[:, step:step + length] * taps[step]
    return result

def left_pad(stream, width):
    return jnp.pad(stream, ((0, 0), (width - 1, 0), (0, 0)))

def state_space(x_conv, b_conv, c_conv, step_size, rate):
    spans = SEQ // BLOCK
    per_group = HEADS // GROUPS
    x_blocks = jnp.moveaxis(x_conv.reshape(BATCH, spans, BLOCK, HEADS, HEAD_DIM), 1, 0)
    b_blocks = jnp.moveaxis(b_conv.reshape(BATCH, spans, BLOCK, GROUPS, STATE), 1, 0)
    c_blocks = jnp.moveaxis(c_conv.reshape(BATCH, spans, BLOCK, GROUPS, STATE), 1, 0)
    step_blocks = jnp.moveaxis(step_size.reshape(BATCH, spans, BLOCK, HEADS), 1, 0)
    lower = lax.iota(jnp.int32, BLOCK)[:, None] >= lax.iota(jnp.int32, BLOCK)[None, :]

    def advance(state, item):
        x_block, b_block, c_block, step_block = item
        b_heads = jnp.repeat(b_block, per_group, axis=2)
        c_heads = jnp.repeat(c_block, per_group, axis=2)
        cum_log = jnp.cumsum(step_block * rate, axis=1)
        log_gap = cum_log[:, :, None, :] - cum_log[:, None, :, :]
        pair_decay = jnp.where(lower[None, :, :, None], jnp.exp(jnp.minimum(log_gap, 0.0)), 0.0)
        scores = jnp.einsum('bihn,bjhn->bijh', c_heads, b_heads, precision=HIGH)
        x_step = x_block * step_block[..., None]
        inner = jnp.einsum('bijh,bjhp->bihp', scores * pair_decay, x_step, precision=HIGH)
        outer = jnp.einsum('bihn,bhpn->bihp', c_heads * jnp.exp(cum_log)[..., None], state, precision=HIGH)
        to_end = jnp.exp(cum_log[:, -1:, :] - cum_log)
        fresh = jnp.einsum('bjhn,bjhp->bhpn', b_heads * to_end[..., None], x_step, precision=HIGH)
        state = state * jnp.exp(cum_log[:, -1, :])[:, :, None, None] + fresh
        return (state, inner + outer)
    start_state = jnp.zeros((BATCH, HEADS, HEAD_DIM, STATE), jnp.float32)
    _, outputs = lax.scan(advance, start_state, (x_blocks, b_blocks, c_blocks, step_blocks))
    return jnp.moveaxis(outputs, 0, 1).reshape(BATCH, SEQ, HEADS * HEAD_DIM)

def reference(tokens, norm_gain, w_z, w_x, w_b, w_c, w_dt, w_gate, w_scb, w_scc, w_scx, conv_x, conv_b, conv_c, conv_sc, dt_bias, decay_log, group_gain, span_shift, w_out):
    rows = tokens.astype(jnp.float32)
    inverse_rms = lax.rsqrt(lax.optimization_barrier(jnp.mean(rows * rows, axis=-1, keepdims=True)) + EPS)
    normed = (rows * inverse_rms * norm_gain).astype(jnp.bfloat16).reshape(BATCH * SEQ, D)

    def project(weight):
        product = jnp.dot(normed, weight, preferred_element_type=jnp.float32)
        return product.astype(jnp.bfloat16).reshape(BATCH, SEQ, weight.shape[1])
    z_stream = project(w_z)
    x_stream = project(w_x)
    b_stream = project(w_b)
    c_stream = project(w_c)
    scb_stream = project(w_scb)
    scc_stream = project(w_scc)
    scx_stream = project(w_scx)
    dt_pre = jnp.dot(normed, w_dt, preferred_element_type=jnp.float32).reshape(BATCH, SEQ, HEADS)
    gate_pre = jnp.dot(normed, w_gate.reshape(D, 2 * HEADS), preferred_element_type=jnp.float32).reshape(BATCH, SEQ, 2, HEADS)
    ssd_width = conv_x.shape[0]
    sc_width = conv_sc.shape[0]
    x_conv = jax.nn.silu(causal_taps(left_pad(x_stream.astype(jnp.float32), ssd_width), conv_x))
    b_conv = jax.nn.silu(causal_taps(left_pad(b_stream.astype(jnp.float32), ssd_width), conv_b))
    c_conv = jax.nn.silu(causal_taps(left_pad(c_stream.astype(jnp.float32), ssd_width), conv_c))
    shift = jnp.repeat(span_shift, BLOCK, axis=1)[:, :, None]
    step_size = jax.nn.softplus(dt_pre + dt_bias + shift)
    rate = -jnp.exp(decay_log)
    core = state_space(x_conv, b_conv, c_conv, step_size, rate)
    gated = core * jax.nn.silu(z_stream.astype(jnp.float32))
    grouped = gated.reshape(BATCH, SEQ, GROUPS, INNER // GROUPS)
    grouped = grouped * lax.rsqrt(lax.optimization_barrier(jnp.mean(grouped * grouped, axis=-1, keepdims=True)) + EPS)
    ssd_out = grouped.reshape(BATCH, SEQ, INNER) * group_gain
    short_in = scc_stream.astype(jnp.float32) * scx_stream.astype(jnp.float32)
    short_out = scb_stream.astype(jnp.float32) * causal_taps(left_pad(short_in, sc_width), conv_sc)
    gates = jax.nn.sigmoid(gate_pre)
    ssd_gate = jnp.repeat(gates[:, :, 0, :], HEAD_DIM, axis=2)
    short_gate = jnp.repeat(gates[:, :, 1, :], HEAD_DIM, axis=2)
    merged = (ssd_gate * ssd_out + short_gate * short_out).astype(jnp.bfloat16).reshape(BATCH * SEQ, INNER)
    mixed = jnp.zeros((BATCH * SEQ, D), jnp.float32)
    for index in range(INNER // SHARE):
        lo_col = index * SHARE
        partial_value = lax.dot_general(merged[:, lo_col:lo_col + SHARE], w_out[:, lo_col:lo_col + SHARE], (((1,), (1,)), ((), ())), preferred_element_type=jnp.float32)
        mixed = mixed + lax.optimization_barrier(partial_value.astype(jnp.bfloat16)).astype(jnp.float32)
    return mixed.astype(jnp.bfloat16).reshape(BATCH, SEQ, D)
```

```python
import functools

import jax
import jax.numpy as jnp
from jax import lax
from jax.experimental import pallas as pl
from jax.experimental.pallas import tpu as pltpu
from jax.sharding import PartitionSpec as P

HEAD_DIM = 64
STATE = 64
BLOCK = 64
EDGE = 8
EPS = 1.0
HIGH = lax.Precision.HIGHEST
F32 = jnp.float32
BF16 = jnp.bfloat16


def silu(v):
    return v / (1.0 + jnp.exp(-v))


def by_columns(w, size):
    rows, cols = w.shape
    return jnp.moveaxis(w.reshape(rows, size, cols // size), 1, 0)


def dot(a, b, contract=((1,), (0,))):
    return lax.dot_general(a, b, (contract, ((), ())), preferred_element_type=F32)


def scan_kernel(taps, heads, xbc_ref, taps_ref, step_ref, cum_ref, cumt_ref, inner_ref, c_ref, state_ref):
    length = inner_ref.shape[1]
    width = heads * HEAD_DIM
    stream = xbc_ref[0].astype(F32)
    conv = stream[EDGE - taps + 1 : EDGE - taps + 1 + length] * taps_ref[0:1]
    for k in range(1, taps):
        lo = EDGE - taps + 1 + k
        conv = conv + stream[lo : lo + length] * taps_ref[k : k + 1]
    conv = silu(conv)
    b = conv[:, width : width + STATE].astype(BF16)
    c = conv[:, width + STATE :].astype(BF16)
    c_ref[0] = c
    scores = dot(c, b, ((1,), (1,)))
    rows = lax.broadcasted_iota(jnp.int32, (length, length), 0)
    cols = lax.broadcasted_iota(jnp.int32, (length, length), 1)
    lower = rows >= cols
    for h in range(heads):
        cum = cum_ref[0, :, h : h + 1]
        gap = cum - cumt_ref[0, h : h + 1, :]
        decay = jnp.where(lower, jnp.exp(jnp.minimum(gap, 0.0)), 0.0)
        x_step = conv[:, h * HEAD_DIM : (h + 1) * HEAD_DIM] * step_ref[0, :, h : h + 1]
        inner_ref[0, :, h * HEAD_DIM : (h + 1) * HEAD_DIM] = dot((scores * decay).astype(BF16), x_step.astype(BF16))
        to_end = jnp.exp(cum[length - 1 : length] - cum)
        state_ref[0, h] = dot((x_step * to_end).astype(BF16), b, ((0,), (0,))).astype(BF16)


def merge_kernel(
    taps, heads, rest_ref, taps_ref, inner_ref, c_ref, cum_ref, prefix_ref, gate_ref, gain_ref, out_ref
):
    length = inner_ref.shape[1]
    width = heads * HEAD_DIM
    z = rest_ref[0, EDGE:, 0:width].astype(F32)
    scb = rest_ref[0, EDGE:, width : 2 * width].astype(F32)
    short_in = rest_ref[0, :, 2 * width : 3 * width].astype(F32) * rest_ref[0, :, 3 * width : 4 * width].astype(F32)
    first = EDGE - taps + 1
    conv = short_in[first : first + length] * taps_ref[0:1]
    for k in range(1, taps):
        conv = conv + short_in[first + k : first + k + length] * taps_ref[k : k + 1]
    short_out = scb * conv
    c = c_ref[0].astype(F32)
    outer = []
    for h in range(heads):
        scaled = (c * jnp.exp(cum_ref[0, :, h : h + 1])).astype(BF16)
        outer.append(dot(scaled, prefix_ref[0, h], ((1,), (1,))))
    core = inner_ref[0] + jnp.concatenate(outer, axis=1)
    gated = core * silu(z)
    scale = lax.rsqrt(jnp.mean(gated * gated, axis=1, keepdims=True) + EPS)
    ssd_out = gated * scale * gain_ref[...]
    gates = jax.nn.sigmoid(gate_ref[0])
    spread = lambda lo: jnp.concatenate(
        [jnp.broadcast_to(gates[:, lo + h : lo + h + 1], (length, HEAD_DIM)) for h in range(heads)], axis=1
    )
    out_ref[0] = (spread(0) * ssd_out + spread(heads) * short_out).astype(out_ref.dtype)


def whole(shape):
    return pl.BlockSpec(shape, lambda s: (0,) * len(shape))


def one(shape):
    return pl.BlockSpec((1, *shape), lambda s: (s,) + (0,) * len(shape))


def body(
    tokens,
    norm_gain,
    w_z,
    w_x,
    w_b,
    w_c,
    w_dt,
    w_gate,
    w_scb,
    w_scc,
    w_scx,
    conv_x,
    conv_b,
    conv_c,
    conv_sc,
    dt_bias,
    decay_log,
    group_gain,
    span_shift,
    w_out,
):
    sp, fs, tp = (lax.axis_size(a) for a in ("sp", "fs", "tp"))
    here_sp, here_fs = lax.axis_index("sp"), lax.axis_index("fs")
    own = tokens[0]
    length, half = own.shape
    heads = dt_bias.shape[0] // fs
    width = heads * HEAD_DIM

    def mine(a, dim):
        size = a.shape[dim] // fs
        return lax.dynamic_slice_in_dim(a, here_fs * size, size, dim)

    def exchanged(weights):
        packed = jnp.concatenate([by_columns(w, fs) for w in weights], axis=2)
        got = lax.all_to_all(packed, "fs", split_axis=0, concat_axis=0, tiled=True)
        return got.reshape(-1, got.shape[2])

    first = exchanged((w_x, w_b, w_c))
    rest = exchanged((w_z, w_scb, w_scc, w_scx, w_out))

    before = lax.ppermute(own[length - EDGE :], "sp", [(i, i + 1) for i in range(sp - 1)])
    block = jnp.concatenate([before, own], axis=0)
    shift = jnp.repeat(span_shift[0], BLOCK)
    block = lax.all_to_all(jnp.broadcast_to(block, (fs, *block.shape)), "fs", 0, 0, tiled=True)
    block = lax.all_to_all(jnp.broadcast_to(block, (tp, *block.shape)), "tp", 0, 0, tiled=True)
    shifts = lax.all_gather(shift, "fs")

    full_first = lax.all_gather(first, "sp", axis=0, tiled=True)
    full_rest = lax.all_gather(rest, "sp", axis=0, tiled=True)

    rows = jnp.concatenate([block[k] for k in range(tp)], axis=2).astype(F32)
    inverse_rms = lax.rsqrt(jnp.mean(rows * rows, axis=2, keepdims=True) + EPS)
    normed = (rows * inverse_rms * norm_gain).astype(BF16).reshape(-1, tp * half)

    narrow = jnp.concatenate([mine(w_dt, 1)] + [mine(w_gate[:, k], 1) for k in range(2)], axis=1)
    small = dot(normed, narrow).reshape(fs, EDGE + length, -1)[:, EDGE:]
    gate_pre = small[:, :, heads:]
    step = jax.nn.softplus(small[:, :, :heads] + mine(dt_bias, 0) + shifts[:, :, None])
    rate = -jnp.exp(mine(decay_log, 0))
    log_step = step * rate
    tri = (lax.iota(jnp.int32, length)[:, None] >= lax.iota(jnp.int32, length)[None, :]).astype(F32)
    cum = jnp.einsum("ij,sjh->sih", tri, log_step, precision=HIGH)
    cum_t = jnp.einsum("ij,sjh->shi", tri, log_step, precision=HIGH)
    total_log = cum_t[:, :, length - 1].reshape(-1)

    xbc = dot(normed, full_first).astype(BF16).reshape(fs, EDGE + length, -1)
    taps_xbc = jnp.concatenate([mine(conv_x, 1), mine(conv_b, 1), mine(conv_c, 1)], axis=1)
    taps = taps_xbc.shape[0]
    inner, c_conv, state = pl.pallas_call(
        functools.partial(scan_kernel, taps, heads),
        grid=(fs,),
        in_specs=[
            one(xbc.shape[1:]),
            whole(taps_xbc.shape),
            one(step.shape[1:]),
            one(cum.shape[1:]),
            one(cum_t.shape[1:]),
        ],
        out_specs=[one((length, width)), one((length, STATE)), one((heads, HEAD_DIM, STATE))],
        out_shape=[
            jax.ShapeDtypeStruct((fs, length, width), F32),
            jax.ShapeDtypeStruct((fs, length, STATE), BF16),
            jax.ShapeDtypeStruct((fs, heads, HEAD_DIM, STATE), BF16),
        ],
    )(xbc, taps_xbc, step, cum, cum_t)

    pairs = fs * heads
    per = pairs // sp
    lanes = 2 * STATE
    flat = state.reshape(pairs, -1, lanes)
    coarse = total_log.astype(BF16)
    left = total_log - coarse.astype(F32)
    middle = left.astype(BF16)
    fine = (left - middle.astype(F32)).astype(BF16)
    logs = jnp.stack([coarse, middle, fine], axis=1)
    logs = jnp.pad(logs, ((0, 0), (0, lanes - 3)))[:, None]
    packed = jnp.concatenate([flat, jnp.pad(logs, ((0, 0), (0, 7), (0, 0)))], axis=1)
    arrived = lax.all_to_all(packed, "sp", 0, 0, tiled=True)
    depth = flat.shape[1]
    logs_all = arrived[:, depth, :3].astype(F32).sum(axis=1).reshape(sp, per)
    source = lax.iota(jnp.int32, sp)
    upto = jnp.einsum("ij,jk->ik", (source[:, None] > source[None, :]).astype(F32), logs_all, precision=HIGH)
    gap = upto[:, None] - (upto + logs_all)[None]
    weight = jnp.where((source[:, None] > source[None, :])[:, :, None], jnp.exp(jnp.minimum(gap, 0.0)), 0.0)
    states_all = arrived[:, :depth].reshape(sp, per, -1).astype(F32)
    prefix = jnp.einsum("zkp,kpe->zpe", weight, states_all, precision=HIGH).astype(BF16)
    prefix = lax.all_to_all(prefix.reshape(sp * per, depth, lanes), "sp", 0, 0, tiled=True)
    prefix = prefix.reshape(fs, heads, HEAD_DIM, STATE)

    full_w = full_rest[:, : 4 * width]
    others = dot(normed, full_w).astype(BF16).reshape(fs, EDGE + length, -1)
    taps_sc = mine(conv_sc, 1)
    gain = mine(group_gain, 0)[None]
    merged = pl.pallas_call(
        functools.partial(merge_kernel, taps_sc.shape[0], heads),
        grid=(fs,),
        in_specs=[
            one(others.shape[1:]),
            whole(taps_sc.shape),
            one(inner.shape[1:]),
            one(c_conv.shape[1:]),
            one(cum.shape[1:]),
            one(prefix.shape[1:]),
            one(gate_pre.shape[1:]),
            whole(gain.shape),
        ],
        out_specs=one((length, width)),
        out_shape=jax.ShapeDtypeStruct((fs, length, width), BF16),
    )(others, taps_sc, inner, c_conv, cum, prefix, gate_pre, gain)

    partial = dot(merged.reshape(-1, width), full_rest[:, 4 * width :], ((1,), (1,))).astype(BF16)
    features = partial.shape[1]
    parts = partial.reshape(fs, tp, length // tp, features)
    parts = jnp.moveaxis(parts, 1, 0)
    parts = lax.all_to_all(parts, "tp", 0, 0, tiled=True).astype(F32).sum(axis=0).astype(BF16)
    mixed = lax.all_to_all(parts, "fs", 0, 0, tiled=True).astype(F32).sum(axis=0).astype(BF16)
    return mixed[None]


def solution(mesh):
    return jax.shard_map(
        body,
        mesh=mesh,
        in_specs=(
            P(("grp", "fs"), "sp", "tp"),
            P(),
            P(("sp", "fs"), "tp"),
            P(("sp", "fs"), "tp"),
            P(("sp", "fs"), "tp"),
            P(("sp", "fs"), "tp"),
            P(None, "tp"),
            P(None, None, "tp"),
            P(("sp", "fs"), "tp"),
            P(("sp", "fs"), "tp"),
            P(("sp", "fs"), "tp"),
            P(None, "tp"),
            P(None, "tp"),
            P(None, "tp"),
            P(None, "tp"),
            P("tp"),
            P("tp"),
            P("tp"),
            P(("grp", "fs"), "sp"),
            P(("sp", "fs"), "tp"),
        ),
        out_specs=P(("grp", "fs"), ("sp", "tp"), None),
        check_vma=False,
    )
```

```python
import functools

import jax
import jax.numpy as jnp
from jax import lax
from jax.experimental import pallas as pl
from jax.experimental.pallas import tpu as pltpu
from jax.sharding import PartitionSpec as P

HEAD_DIM = 64
BLOCK = 64
EDGE = 8
LANES = 128
EPS = 1.0
HIGH = lax.Precision.HIGHEST
F32 = jnp.float32
BF16 = jnp.bfloat16


def silu(v):
    return v / (1.0 + jnp.exp(-v))


def dot(a, b, contract=((1,), (0,))):
    return lax.dot_general(a, b, (contract, ((), ())), preferred_element_type=F32)


def taps_of(extended, taps_ref, count, length):
    first = EDGE - count + 1
    result = extended[first : first + length] * taps_ref[0:1]
    for k in range(1, count):
        result = result + extended[first + k : first + k + length] * taps_ref[k : k + 1]
    return result


def mixer_kernel(
    many, long_taps, short_taps, own_ref, recv_ref, rows_ref, taps_ref, taps_sc_ref, gain_ref, ab_ref, tail_ref, state_ref
):
    length = ab_ref.shape[1] - EDGE
    hd = HEAD_DIM

    @pl.when(pl.program_id(0) == 0)
    def _():
        tail_ref[...] = jnp.zeros_like(tail_ref)
        state_ref[...] = jnp.zeros_like(state_ref)

    lower = lax.broadcasted_iota(jnp.int32, (length, length), 0) >= lax.broadcasted_iota(
        jnp.int32, (length, length), 1
    )
    tail = tail_ref[...]
    state = state_ref[...]
    for k in range(many):
        rows = rows_ref[k]
        cols = rows.T
        step, cum, gate, gate_sc, inverse = (cols[:, i : i + 1] for i in range(5))
        stream = (own_ref[k] + recv_ref[k].astype(F32)) * inverse
        short_in = stream[:, 4 * hd : 5 * hd] * stream[:, 6 * hd : 7 * hd]
        conv = taps_of(jnp.concatenate([tail[:, : 4 * hd], stream[:, : 4 * hd]], axis=0), taps_ref, long_taps, length)
        conv_sc = taps_of(
            jnp.concatenate([tail[:, 4 * hd : 5 * hd], short_in], axis=0), taps_sc_ref, short_taps, length
        )
        tail = jnp.concatenate([stream[length - EDGE :, : 4 * hd], short_in[length - EDGE :], short_in[length - EDGE :]], axis=1)
        conv = silu(conv[:, : 3 * hd])
        x = conv[:, :hd] * step
        b = conv[:, hd : 2 * hd].astype(BF16)
        c = conv[:, 2 * hd : 3 * hd]
        z = stream[:, 3 * hd : 4 * hd]
        scb = stream[:, 5 * hd : 6 * hd]
        scores = dot(c.astype(BF16), b, ((1,), (1,)))
        decay = jnp.where(lower, jnp.exp(jnp.minimum(cum - rows[1:2], 0.0)), 0.0)
        core = dot((scores * decay).astype(BF16), x.astype(BF16))
        core = core + dot((c * jnp.exp(cum)).astype(BF16), state.astype(BF16), ((1,), (1,)))
        last = cum[length - 1 : length]
        fresh = dot((x * jnp.exp(last - cum)).astype(BF16), b, ((0,), (0,)))
        state = state * jnp.exp(last) + fresh
        gated = core * silu(z)
        squares = lax.dot_general(
            jnp.ones((EDGE, hd), F32), gated * gated, (((1,), (1,)), ((), ())), precision=HIGH, preferred_element_type=F32
        )
        coarse = squares.astype(BF16)
        fine = (squares - coarse.astype(F32)).astype(BF16)
        which = lax.broadcasted_iota(jnp.int32, squares.shape, 0)
        packed = jnp.where(which == 0, coarse.astype(F32), jnp.where(which == 1, fine.astype(F32), 0.0))
        both = jnp.concatenate([gated * gain_ref[...] * gate, gate_sc * (scb * conv_sc)], axis=1)
        ab_ref[k] = jnp.concatenate([both, packed], axis=0).astype(BF16)
    tail_ref[...] = tail
    state_ref[...] = state


def merge_kernel(per_group, ab_ref, out_ref):
    count, full = ab_ref.shape[0], ab_ref.shape[1]
    length = full - EDGE
    hd = HEAD_DIM
    ones = jnp.ones((per_group * EDGE, LANES), BF16)
    for g in range(count // per_group):
        squares = jnp.concatenate([ab_ref[g * per_group + k, length:, :] for k in range(per_group)], axis=0)
        mean = dot(squares, ones, ((0,), (0,))) * (1.0 / (per_group * hd))
        scale = lax.rsqrt(mean + EPS)[:, :hd]
        for k in range(0, per_group, 2):
            pair = []
            for j in range(2):
                ab = ab_ref[g * per_group + k + j, :length, :].astype(F32)
                pair.append(ab[:, :hd] * scale + ab[:, hd:])
            lo = (g * per_group + k) * hd
            out_ref[:, lo : lo + 2 * hd] = jnp.concatenate(pair, axis=1).astype(out_ref.dtype)


def gathered(x, axis):
    return lax.all_gather(x, axis)


def body(
    tokens,
    norm_gain,
    w_z,
    w_x,
    w_b,
    w_c,
    w_dt,
    w_gate,
    w_scb,
    w_scc,
    w_scx,
    conv_x,
    conv_b,
    conv_c,
    conv_sc,
    dt_bias,
    decay_log,
    group_gain,
    span_shift,
    w_out,
):
    sp, fs, tp = (lax.axis_size(a) for a in ("sp", "fs", "tp"))
    here, side = lax.axis_index("sp"), lax.axis_index("tp")
    own = tokens[0]
    length, half = own.shape
    hd = HEAD_DIM
    heads = dt_bias.shape[0]
    share = heads // sp
    groups = conv_b.shape[1] // hd
    per_group = heads // groups
    depth = w_x.shape[0]

    def cut(w):
        return jnp.moveaxis(w.reshape(w.shape[0], heads, hd), 1, 0)

    def cut_group(w):
        return jnp.repeat(jnp.moveaxis(w.reshape(w.shape[0], groups, hd), 1, 0), per_group, axis=0)

    packed = jnp.concatenate(
        [cut(w_x), cut_group(w_b), cut_group(w_c), cut(w_z), cut(w_scc), cut(w_scb), cut(w_scx)], axis=2
    )
    packed = jnp.pad(packed, ((0, 0), (0, 0), (0, hd)))
    cols = packed.shape[2]
    got = lax.all_to_all(packed, "sp", 0, 0, tiled=True)

    payload = jnp.concatenate([own, w_out], axis=0)
    everything = gathered(payload, "sp")

    halves = got.reshape(tp, (sp // tp) * depth, cols)
    halves = jnp.broadcast_to(halves, (fs, *halves.shape)).reshape(fs * tp, -1, cols)
    halves = lax.all_to_all(halves, ("fs", "tp"), 0, 0, tiled=True)
    weights = halves.reshape(fs, tp, sp // tp, depth, cols).transpose(1, 2, 0, 3, 4).reshape(tp, half, cols)
    gain = lax.dynamic_slice_in_dim(norm_gain, side * half, half)
    weights = (weights.astype(F32) * gain[:, None]).astype(BF16)
    w_mine = lax.dynamic_index_in_dim(weights, side, 0, keepdims=False)
    w_other = lax.dynamic_index_in_dim(weights, (tp - 1) - side, 0, keepdims=False)

    pair = lax.all_to_all(jnp.broadcast_to(own, (tp, *own.shape)), "tp", 0, 0, tiled=True)
    rows = jnp.concatenate([pair[k] for k in range(tp)], axis=1).astype(F32)
    inverse_rms = lax.rsqrt(jnp.mean(rows * rows, axis=1, keepdims=True) + EPS)
    normed = (rows * inverse_rms * norm_gain).astype(BF16)
    narrow = jnp.concatenate([w_dt, w_gate.reshape(w_gate.shape[0], -1)], axis=1)
    small = dot(narrow, normed, ((0,), (1,)))
    shift = jnp.repeat(span_shift[0], BLOCK)
    step = jax.nn.softplus(small[:heads] + dt_bias[:, None] + shift[None, :])
    rate = -jnp.exp(decay_log)[:, None]
    upper = (lax.iota(jnp.int32, length)[:, None] <= lax.iota(jnp.int32, length)[None, :]).astype(F32)
    cum = jnp.dot(step * rate, upper, precision=HIGH)
    gates = jax.nn.sigmoid(small[heads:])
    inverse_rows = jnp.broadcast_to(inverse_rms[:, 0][None, :], (heads, length))
    info = jnp.stack([step, cum, gates[:heads], gates[heads:], inverse_rows], axis=1)
    info = jnp.pad(info, ((0, 0), (0, EDGE - info.shape[1]), (0, 0)))
    info = lax.all_to_all(info, "sp", 0, 0, tiled=True)

    flat = everything.reshape(-1, half)
    other = dot(flat, w_other).astype(BF16)
    arrived = lax.ppermute(other, "tp", [(i, tp - 1 - i) for i in range(tp)])
    mine = dot(flat, w_mine)
    mine = mine.reshape(sp, -1, cols)
    arrived = arrived.reshape(sp, -1, cols)

    def head_of(a, dim):
        return lax.dynamic_slice_in_dim(a, here * share * hd, share * hd, dim)

    def group_of(a):
        return lax.dynamic_slice_in_dim(a, (here * share // per_group) * hd, hd, 1)

    taps = jnp.concatenate([head_of(conv_x, 1), group_of(conv_b), group_of(conv_c)], axis=1)
    taps = jnp.pad(taps, ((0, 0), (0, hd)))
    taps_sc = head_of(conv_sc, 1)
    own_gain = head_of(group_gain, 0)[None]
    many = 2
    block = lambda shape: pl.BlockSpec((many, *shape), lambda i: (i,) + (0,) * len(shape))
    whole = lambda a: pl.BlockSpec(a.shape, lambda i: (0,) * a.ndim)
    ab = pl.pallas_call(
        functools.partial(mixer_kernel, many, taps.shape[0], taps_sc.shape[0]),
        grid=(sp // many,),
        in_specs=[
            block((length, cols)),
            block((length, cols)),
            block((EDGE, length)),
            whole(taps),
            whole(taps_sc),
            whole(own_gain),
        ],
        out_specs=block((length + EDGE, 2 * hd)),
        out_shape=jax.ShapeDtypeStruct((sp, length + EDGE, 2 * hd), BF16),
        scratch_shapes=[pltpu.VMEM((EDGE, 6 * hd), F32), pltpu.VMEM((hd, hd), F32)],
        name="mixer",
    )(mine, arrived, info, taps, taps_sc, own_gain)

    w_rows = everything[:, length:].reshape(-1, half)
    w_all = lax.all_to_all(jnp.broadcast_to(w_rows, (fs, *w_rows.shape)), "fs", 0, 0, tiled=True)
    w_all = w_all.reshape(fs, sp, depth, half).transpose(1, 0, 2, 3).reshape(-1, half)

    ab = lax.all_to_all(ab, "sp", 0, 0, tiled=True)
    merged = pl.pallas_call(
        functools.partial(merge_kernel, per_group),
        out_shape=jax.ShapeDtypeStruct((length, sp * hd), BF16),
        name="merge",
    )(ab)
    partial = dot(merged, w_all, ((1,), (1,))).astype(BF16)
    parts = partial.reshape(tp, length // tp, partial.shape[1])
    parts = lax.all_to_all(parts, "tp", 0, 0, tiled=True)
    return parts.astype(F32).sum(axis=0).astype(BF16)[None]


def solution(mesh):
    return jax.shard_map(
        body,
        mesh=mesh,
        in_specs=(
            P(("grp", "fs"), "sp", "tp"),
            P(),
            P(("sp", "fs"), "tp"),
            P(("sp", "fs"), "tp"),
            P(("sp", "fs"), "tp"),
            P(("sp", "fs"), "tp"),
            P(None, "tp"),
            P(None, None, "tp"),
            P(("sp", "fs"), "tp"),
            P(("sp", "fs"), "tp"),
            P(("sp", "fs"), "tp"),
            P(None, "tp"),
            P(None, "tp"),
            P(None, "tp"),
            P(None, "tp"),
            P("tp"),
            P("tp"),
            P("tp"),
            P(("grp", "fs"), "sp"),
            P(("sp", "fs"), "tp"),
        ),
        out_specs=P(("grp", "fs"), ("sp", "tp"), None),
        check_vma=False,
    )
```

```python
import functools

import jax
import jax.numpy as jnp
from jax import lax
from jax.experimental import pallas as pl
from jax.experimental.pallas import tpu as pltpu
from jax.sharding import PartitionSpec as P


HEAD_DIM = 64
BLOCK = 64
EDGE = 8
LANES = 128
HOLD = 4
EPS = 1.0
HIGH = lax.Precision.HIGHEST
F32 = jnp.float32
BF16 = jnp.bfloat16


def silu(v):
    return v / (1.0 + jnp.exp(-v))


def dot(a, b, contract=((1,), (0,))):
    return lax.dot_general(a, b, (contract, ((), ())), preferred_element_type=F32)


def taps_of(extended, taps_ref, count, length):
    first = EDGE - count + 1
    result = extended[first : first + length] * taps_ref[0:1]
    for k in range(1, count):
        result = result + extended[first + k : first + k + length] * taps_ref[k : k + 1]
    return result


def mixer_kernel(
    many, long_taps, short_taps, own_ref, recv_ref, rows_ref, taps_ref, taps_sc_ref, gain_ref, ab_ref, tail_ref, state_ref
):
    length = ab_ref.shape[1] - EDGE
    hd = HEAD_DIM

    @pl.when(pl.program_id(0) == 0)
    def _():
        tail_ref[...] = jnp.zeros_like(tail_ref)
        state_ref[...] = jnp.zeros_like(state_ref)

    lower = lax.broadcasted_iota(jnp.int32, (length, length), 0) >= lax.broadcasted_iota(
        jnp.int32, (length, length), 1
    )
    tail = tail_ref[...]
    state = state_ref[...]
    for k in range(many):
        rows = rows_ref[k]
        cols = rows.T
        step, cum, gate, gate_sc, inverse = (cols[:, i : i + 1] for i in range(5))
        stream = (own_ref[k].astype(F32) + recv_ref[k].astype(F32)) * inverse
        short_in = stream[:, 4 * hd : 5 * hd] * stream[:, 6 * hd : 7 * hd]
        conv = taps_of(jnp.concatenate([tail[:, : 4 * hd], stream[:, : 4 * hd]], axis=0), taps_ref, long_taps, length)
        conv_sc = taps_of(
            jnp.concatenate([tail[:, 4 * hd : 5 * hd], short_in], axis=0), taps_sc_ref, short_taps, length
        )
        tail = jnp.concatenate([stream[length - EDGE :, : 4 * hd], short_in[length - EDGE :], short_in[length - EDGE :]], axis=1)
        conv = silu(conv[:, : 3 * hd])
        x = conv[:, :hd] * step
        b = conv[:, hd : 2 * hd].astype(BF16)
        c = conv[:, 2 * hd : 3 * hd]
        z = stream[:, 3 * hd : 4 * hd]
        scb = stream[:, 5 * hd : 6 * hd]
        scores = dot(c.astype(BF16), b, ((1,), (1,)))
        decay = jnp.where(lower, jnp.exp(jnp.minimum(cum - rows[1:2], 0.0)), 0.0)
        core = dot((scores * decay).astype(BF16), x.astype(BF16))
        core = core + dot((c * jnp.exp(cum)).astype(BF16), state.astype(BF16), ((1,), (1,)))
        last = cum[length - 1 : length]
        fresh = dot((x * jnp.exp(last - cum)).astype(BF16), b, ((0,), (0,)))
        state = state * jnp.exp(last) + fresh
        gated = core * silu(z)
        squares = lax.dot_general(
            jnp.ones((EDGE, hd), F32), gated * gated, (((1,), (1,)), ((), ())), precision=HIGH, preferred_element_type=F32
        )
        coarse = squares.astype(BF16)
        fine = (squares - coarse.astype(F32)).astype(BF16)
        which = lax.broadcasted_iota(jnp.int32, squares.shape, 0)
        packed = jnp.where(which == 0, coarse.astype(F32), jnp.where(which == 1, fine.astype(F32), 0.0))
        both = jnp.concatenate([gated * gain_ref[...] * gate, gate_sc * (scb * conv_sc)], axis=1)
        ab_ref[k] = jnp.concatenate([both, packed], axis=0).astype(BF16)
    tail_ref[...] = tail
    state_ref[...] = state


def merge_kernel(per_group, ab_ref, out_ref):
    count, full = ab_ref.shape[0], ab_ref.shape[1]
    length = full - EDGE
    hd = HEAD_DIM
    ones = jnp.ones((per_group * EDGE, LANES), BF16)
    for g in range(count // per_group):
        squares = jnp.concatenate([ab_ref[g * per_group + k, length:, :] for k in range(per_group)], axis=0)
        mean = dot(squares, ones, ((0,), (0,))) * (1.0 / (per_group * hd))
        scale = lax.rsqrt(mean + EPS)[:, :hd]
        for k in range(0, per_group, 2):
            pair = []
            for j in range(2):
                ab = ab_ref[g * per_group + k + j, :length, :].astype(F32)
                pair.append(ab[:, :hd] * scale + ab[:, hd:])
            lo = (g * per_group + k) * hd
            out_ref[:, lo : lo + 2 * hd] = jnp.concatenate(pair, axis=1).astype(out_ref.dtype)


def pack_kernel(per_group, x_ref, b_ref, c_ref, z_ref, scc_ref, scb_ref, scx_ref, out_ref):
    hd = HEAD_DIM
    for h in range(out_ref.shape[0]):
        g = h // per_group
        own = slice(h * hd, (h + 1) * hd)
        group = slice(g * hd, (g + 1) * hd)
        parts = [x_ref[:, own], b_ref[:, group], c_ref[:, group], z_ref[:, own]]
        parts += [scc_ref[:, own], scb_ref[:, own], scx_ref[:, own]]
        parts += [jnp.zeros_like(parts[0])]
        out_ref[h] = jnp.concatenate(parts, axis=1)


def project_kernel(count, parts, batch, tile, order_ref, *refs):
    pieces = refs[: count * parts]
    w_ref, mine_ref, other_ref, rows_ref = refs[count * parts :]
    length, cols = mine_ref.shape[1:]
    extra = rows_ref.shape[1]
    width = pieces[0].shape[1]
    for g in range(0, count, batch):
        group = pieces[g * parts : (g + batch) * parts]
        places = [order_ref[g + j] for j in range(batch)]

        @pl.loop(0, cols // tile)
        def _(step):
            at = pl.multiple_of(step * tile, tile)
            for side, out_ref in enumerate((mine_ref, other_ref)):
                column = pl.ds(pl.multiple_of(side * cols + step * tile, tile), tile)
                total = 0.0
                for p in range(parts):
                    left = jnp.concatenate([group[j * parts + p][:length, :] for j in range(batch)], axis=0)
                    total = total + dot(left, w_ref[p * width : (p + 1) * width, column])
                for j in range(batch):
                    out_ref[places[j], :, pl.ds(at, tile)] = total[j * length : (j + 1) * length].astype(BF16)

        for j in range(batch):
            for p in range(parts):
                rows_ref[places[j], :, p * width : (p + 1) * width] = group[j * parts + p][length : length + extra, :]


def ring(x, parts):
    sp, tp = lax.axis_size("sp"), lax.axis_size("tp")
    here, side = lax.axis_index("sp"), lax.axis_index("tp")
    along = [(i * tp + c, (i + 1 - 2 * c) % sp * tp + c) for i in range(sp) for c in range(tp)]
    against = [(b, a) for a, b in along]
    sign = 1 - 2 * side
    width = x.shape[1] // parts
    start = [x[:, p * width : (p + 1) * width] for p in range(parts)]
    ahead, behind = list(start), list(start)
    pieces, order = [start], [here]
    for s in range(1, sp // 2 + 1):
        both = s < sp - sp // 2
        ahead = [lax.ppermute(a, ("sp", "tp"), along) for a in ahead]
        if both:
            behind = [lax.ppermute(a, ("sp", "tp"), against) for a in behind]
            for p in range(parts):
                ahead[p], behind[p] = lax.optimization_barrier((ahead[p], behind[p]))
        pieces.append(list(ahead))
        order.append((here - sign * s) % sp)
        if both:
            pieces.append(list(behind))
            order.append((here + sign * s) % sp)
    return [p for block in pieces for p in block], jnp.stack(order)


def body(
    tokens,
    norm_gain,
    w_z,
    w_x,
    w_b,
    w_c,
    w_dt,
    w_gate,
    w_scb,
    w_scc,
    w_scx,
    conv_x,
    conv_b,
    conv_c,
    conv_sc,
    dt_bias,
    decay_log,
    group_gain,
    span_shift,
    w_out,
):
    sp, fs, tp = (lax.axis_size(a) for a in ("sp", "fs", "tp"))
    here, side = lax.axis_index("sp"), lax.axis_index("tp")
    own = tokens[0]
    length, half = own.shape
    hd = HEAD_DIM
    heads = dt_bias.shape[0]
    share = heads // sp
    groups = conv_b.shape[1] // hd
    per_group = heads // groups
    depth = depth_own = w_x.shape[0]

    packed = pl.pallas_call(
        functools.partial(pack_kernel, per_group),
        out_shape=jax.ShapeDtypeStruct((sp, depth_own, 8 * hd), BF16),
        name="pack",
    )(w_x, w_b, w_c, w_z, w_scc, w_scb, w_scx)
    cols = packed.shape[2]
    got = lax.all_to_all(packed, "sp", 0, 0, tiled=True)

    payload = jnp.concatenate([own, w_out], axis=0)
    parts = 2
    pieces, order = ring(payload, parts)
    hold = (HOLD * 2 - 1) * parts

    got, *pieces[hold : hold + parts] = lax.optimization_barrier((got, *pieces[hold : hold + parts]))
    halves = got.reshape(tp, (sp // tp) * depth, cols)
    halves = jnp.broadcast_to(halves, (fs, *halves.shape)).reshape(fs * tp, -1, cols)
    halves = lax.all_to_all(halves, ("fs", "tp"), 0, 0, tiled=True)
    weights = halves.reshape(fs, tp, sp // tp, depth, cols).transpose(1, 2, 0, 3, 4).reshape(tp, half, cols)
    gain = lax.dynamic_slice_in_dim(norm_gain, side * half, half)
    weights = (weights.astype(F32) * gain[:, None]).astype(BF16)
    w_mine = lax.dynamic_index_in_dim(weights, side, 0, keepdims=False)
    w_other = lax.dynamic_index_in_dim(weights, (tp - 1) - side, 0, keepdims=False)

    swap = [(i, tp - 1 - i) for i in range(tp)]
    partner = lax.ppermute(own, "tp", swap)
    rows = jnp.where(
        side == 0, jnp.concatenate([own, partner], axis=1), jnp.concatenate([partner, own], axis=1)
    ).astype(F32)
    inverse_rms = lax.rsqrt(jnp.mean(rows * rows, axis=1, keepdims=True) + EPS)
    normed = (rows * inverse_rms * norm_gain).astype(BF16)
    narrow = jnp.concatenate([w_dt, w_gate.reshape(w_gate.shape[0], -1)], axis=1)
    small = dot(narrow, normed, ((0,), (1,)))
    shift = jnp.repeat(span_shift[0], BLOCK)
    step = jax.nn.softplus(small[:heads] + dt_bias[:, None] + shift[None, :])
    rate = -jnp.exp(decay_log)[:, None]
    upper = (lax.iota(jnp.int32, length)[:, None] <= lax.iota(jnp.int32, length)[None, :]).astype(F32)
    cum = jnp.dot(step * rate, upper, precision=HIGH)
    gates = jax.nn.sigmoid(small[heads:])
    inverse_rows = jnp.broadcast_to(inverse_rms[:, 0][None, :], (heads, length))
    info = jnp.stack([step, cum, gates[:heads], gates[heads:], inverse_rows], axis=1)
    info = jnp.pad(info, ((0, 0), (0, EDGE - info.shape[1]), (0, 0)))
    info = lax.all_to_all(info, "sp", 0, 0, tiled=True)

    vmem = pl.BlockSpec(memory_space=pltpu.VMEM)
    w_both = jnp.concatenate([w_mine, w_other], axis=1)
    project = pl.pallas_call(
        functools.partial(project_kernel, sp, parts, 4, 256),
        in_specs=[pl.BlockSpec(memory_space=pltpu.SMEM)] + [vmem] * (len(pieces) + 1),
        out_specs=[vmem] * 3,
        out_shape=[
            jax.ShapeDtypeStruct((sp, length, cols), BF16),
            jax.ShapeDtypeStruct((sp, length, cols), BF16),
            jax.ShapeDtypeStruct((sp, depth, half), BF16),
        ],
        name="project",
    )
    mine, other, w_rows = project(order, *pieces, w_both)
    arrived = lax.ppermute(other, "tp", swap)

    def head_of(a, dim):
        return lax.dynamic_slice_in_dim(a, here * share * hd, share * hd, dim)

    def group_of(a):
        return lax.dynamic_slice_in_dim(a, (here * share // per_group) * hd, hd, 1)

    taps = jnp.concatenate([head_of(conv_x, 1), group_of(conv_b), group_of(conv_c)], axis=1)
    taps = jnp.pad(taps, ((0, 0), (0, hd)))
    taps_sc = head_of(conv_sc, 1)
    own_gain = head_of(group_gain, 0)[None]
    many = 2
    block = lambda shape: pl.BlockSpec((many, *shape), lambda i: (i,) + (0,) * len(shape))
    whole = lambda a: pl.BlockSpec(a.shape, lambda i: (0,) * a.ndim)
    mixer = pl.pallas_call(
        functools.partial(mixer_kernel, many, taps.shape[0], taps_sc.shape[0]),
        grid=(sp // many,),
        in_specs=[
            block((length, cols)),
            block((length, cols)),
            block((EDGE, length)),
            whole(taps),
            whole(taps_sc),
            whole(own_gain),
        ],
        out_specs=block((length + EDGE, 2 * hd)),
        out_shape=jax.ShapeDtypeStruct((sp, length + EDGE, 2 * hd), BF16),
        scratch_shapes=[pltpu.VMEM((EDGE, 6 * hd), F32), pltpu.VMEM((hd, hd), F32)],
        name="mixer",
    )
    ab = mixer(mine, arrived, info, taps, taps_sc, own_gain)

    w_rows = w_rows.reshape(-1, half)
    fs_here = lax.axis_index("fs")
    w_parts = [w_rows]
    for k in range(1, fs):
        w_parts.append(lax.ppermute(w_rows, "fs", [(i, (i + k) % fs) for i in range(fs)]))
    w_parts = jnp.stack(w_parts)
    w_all = [lax.dynamic_index_in_dim(w_parts, (fs_here - k) % fs, 0, keepdims=False) for k in range(fs)]
    w_all = jnp.stack([w.reshape(sp, depth, half) for w in w_all], axis=1).reshape(-1, half)
    ab = lax.all_to_all(ab, "sp", 0, 0, tiled=True)
    merged = pl.pallas_call(
        functools.partial(merge_kernel, per_group),
        out_shape=jax.ShapeDtypeStruct((length, sp * hd), BF16),
        name="merge",
    )(ab)
    partial = dot(merged, w_all, ((1,), (1,))).astype(BF16)
    parts = partial.reshape(tp, length // tp, partial.shape[1])
    parts = lax.all_to_all(parts, "tp", 0, 0, tiled=True)
    return parts.astype(F32).sum(axis=0).astype(BF16)[None]


def solution(mesh):
    return mapped(mesh)


def mapped(mesh):
    return jax.shard_map(
        body,
        mesh=mesh,
        in_specs=(
            P(("grp", "fs"), "sp", "tp"),
            P(),
            P(("sp", "fs"), "tp"),
            P(("sp", "fs"), "tp"),
            P(("sp", "fs"), "tp"),
            P(("sp", "fs"), "tp"),
            P(None, "tp"),
            P(None, None, "tp"),
            P(("sp", "fs"), "tp"),
            P(("sp", "fs"), "tp"),
            P(("sp", "fs"), "tp"),
            P(None, "tp"),
            P(None, "tp"),
            P(None, "tp"),
            P(None, "tp"),
            P("tp"),
            P("tp"),
            P("tp"),
            P(("grp", "fs"), "sp"),
            P(("sp", "fs"), "tp"),
        ),
        out_specs=P(("grp", "fs"), ("sp", "tp"), None),
        check_vma=False,
    )
```

```python
import functools

import jax
import jax.numpy as jnp
from jax import lax
from jax.experimental import pallas as pl
from jax.experimental.pallas import tpu as pltpu
from jax.sharding import PartitionSpec as P


HEAD_DIM = 64
BLOCK = 64
EDGE = 8
LANES = 128
HOLD = 4
EPS = 1.0
HIGH = lax.Precision.HIGHEST
F32 = jnp.float32
BF16 = jnp.bfloat16


def silu(v):
    return v / (1.0 + jnp.exp(-v))


def dot(a, b, contract=((1,), (0,))):
    return lax.dot_general(a, b, (contract, ((), ())), preferred_element_type=F32)


def taps_of(extended, taps_ref, count, length):
    first = EDGE - count + 1
    result = extended[first : first + length] * taps_ref[0:1]
    for k in range(1, count):
        result = result + extended[first + k : first + k + length] * taps_ref[k : k + 1]
    return result


def mixer_kernel(
    many, long_taps, short_taps, own_ref, recv_ref, rows_ref, taps_ref, taps_sc_ref, gain_ref, ab_ref, tail_ref, state_ref
):
    length = ab_ref.shape[1] - EDGE
    hd = HEAD_DIM

    @pl.when(pl.program_id(0) == 0)
    def _():
        tail_ref[...] = jnp.zeros_like(tail_ref)
        state_ref[...] = jnp.zeros_like(state_ref)

    lower = lax.broadcasted_iota(jnp.int32, (length, length), 0) >= lax.broadcasted_iota(
        jnp.int32, (length, length), 1
    )
    tail = tail_ref[...]
    state = state_ref[...]
    for k in range(many):
        rows = rows_ref[k]
        cols = rows.T
        step, cum, gate, gate_sc, inverse = (cols[:, i : i + 1] for i in range(5))
        stream = (own_ref[k].astype(F32) + recv_ref[k].astype(F32)) * inverse
        short_in = stream[:, 4 * hd : 5 * hd] * stream[:, 6 * hd : 7 * hd]
        conv = taps_of(jnp.concatenate([tail[:, : 4 * hd], stream[:, : 4 * hd]], axis=0), taps_ref, long_taps, length)
        conv_sc = taps_of(
            jnp.concatenate([tail[:, 4 * hd : 5 * hd], short_in], axis=0), taps_sc_ref, short_taps, length
        )
        tail = jnp.concatenate([stream[length - EDGE :, : 4 * hd], short_in[length - EDGE :], short_in[length - EDGE :]], axis=1)
        conv = silu(conv[:, : 3 * hd])
        x = conv[:, :hd] * step
        b = conv[:, hd : 2 * hd].astype(BF16)
        c = conv[:, 2 * hd : 3 * hd]
        z = stream[:, 3 * hd : 4 * hd]
        scb = stream[:, 5 * hd : 6 * hd]
        scores = dot(c.astype(BF16), b, ((1,), (1,)))
        decay = jnp.where(lower, jnp.exp(jnp.minimum(cum - rows[1:2], 0.0)), 0.0)
        core = dot((scores * decay).astype(BF16), x.astype(BF16))
        core = core + dot((c * jnp.exp(cum)).astype(BF16), state.astype(BF16), ((1,), (1,)))
        last = cum[length - 1 : length]
        fresh = dot((x * jnp.exp(last - cum)).astype(BF16), b, ((0,), (0,)))
        state = state * jnp.exp(last) + fresh
        gated = core * silu(z)
        squares = lax.dot_general(
            jnp.ones((EDGE, hd), F32), gated * gated, (((1,), (1,)), ((), ())), precision=HIGH, preferred_element_type=F32
        )
        coarse = squares.astype(BF16)
        fine = (squares - coarse.astype(F32)).astype(BF16)
        which = lax.broadcasted_iota(jnp.int32, squares.shape, 0)
        packed = jnp.where(which == 0, coarse.astype(F32), jnp.where(which == 1, fine.astype(F32), 0.0))
        both = jnp.concatenate([gated * gain_ref[...] * gate, gate_sc * (scb * conv_sc)], axis=1)
        ab_ref[k] = jnp.concatenate([both, packed], axis=0).astype(BF16)
    tail_ref[...] = tail
    state_ref[...] = state


def merge_kernel(per_group, ab_ref, out_ref):
    count, full = ab_ref.shape[0], ab_ref.shape[1]
    length = full - EDGE
    hd = HEAD_DIM
    ones = jnp.ones((per_group * EDGE, LANES), BF16)
    for g in range(count // per_group):
        squares = jnp.concatenate([ab_ref[g * per_group + k, length:, :] for k in range(per_group)], axis=0)
        mean = dot(squares, ones, ((0,), (0,))) * (1.0 / (per_group * hd))
        scale = lax.rsqrt(mean + EPS)[:, :hd]
        for k in range(0, per_group, 2):
            pair = []
            for j in range(2):
                ab = ab_ref[g * per_group + k + j, :length, :].astype(F32)
                pair.append(ab[:, :hd] * scale + ab[:, hd:])
            lo = (g * per_group + k) * hd
            out_ref[:, lo : lo + 2 * hd] = jnp.concatenate(pair, axis=1).astype(out_ref.dtype)


def pack_kernel(per_group, gain_ref, info_ref, x_ref, b_ref, c_ref, z_ref, scc_ref, scb_ref, scx_ref, out_ref):
    hd = HEAD_DIM
    depth = x_ref.shape[0]
    gain = gain_ref[...]
    scaled = [(ref[...].astype(F32) * gain).astype(BF16) for ref in (x_ref, b_ref, c_ref, z_ref, scc_ref, scb_ref, scx_ref)]
    x, b, c, z, scc, scb, scx = scaled
    for h in range(out_ref.shape[0]):
        g = h // per_group
        own = slice(h * hd, (h + 1) * hd)
        group = slice(g * hd, (g + 1) * hd)
        parts = [x[:, own], b[:, group], c[:, group], z[:, own], scc[:, own], scb[:, own], scx[:, own]]
        parts += [jnp.zeros_like(parts[0])]
        out_ref[h, :depth, :] = jnp.concatenate(parts, axis=1)
        left = info_ref[h]
        split = []
        for _ in range(3):
            part = left.astype(BF16)
            split.append(part)
            left = left - part.astype(F32)
        split.append(jnp.zeros_like(split[0]))
        out_ref[h, depth:, :] = jnp.concatenate(split, axis=1)


def project_kernel(count, parts, rows, tile, order_ref, source_ref, *refs):
    pieces = refs[: count * parts]
    halves_ref, out_ref, tokens_ref, w_ref = refs[count * parts :]
    length, cols = out_ref.shape[1:]
    width = pieces[0].shape[1]
    fs, _, spans, depth, _ = halves_ref.shape
    source = source_ref[0]
    for k in range(count):
        at = pl.multiple_of(order_ref[k] * length, length)
        for p in range(parts):
            tokens_ref[pl.ds(at, length), p * width : (p + 1) * width] = pieces[k * parts + p][:length, :]
    for span in range(spans):
        for f in range(fs):
            lo = (span * fs + f) * depth
            w_ref[lo : lo + depth, :] = halves_ref[f, source, span]

    @pl.loop(0, count * length // rows)
    def _(step):
        left = tokens_ref[pl.ds(pl.multiple_of(step * rows, rows), rows), :]
        for lo in range(0, cols, tile):
            total = dot(left, w_ref[:, lo : lo + tile]).astype(BF16)
            out_ref[pl.ds(step * (rows // length), rows // length), :, lo : lo + tile] = total.reshape(
                rows // length, length, tile
            )


def assemble_kernel(order_ref, place_ref, *refs):
    early, late, out_ref = refs[: (len(refs) - 1) // 2], refs[(len(refs) - 1) // 2 : -1], refs[-1]
    first, depth = early[0].shape[:2]
    for k in range(len(early)):
        for ref, base in ((early[k], 0), (late[k], first)):
            for j in range(ref.shape[0]):
                at = pl.multiple_of((order_ref[base + j] * len(early) + place_ref[k]) * depth, depth)
                out_ref[pl.ds(at, depth), :] = ref[j]


def ring(x, parts):
    sp, tp = lax.axis_size("sp"), lax.axis_size("tp")
    here, side = lax.axis_index("sp"), lax.axis_index("tp")
    along = [(i * tp + c, (i + 1 - 2 * c) % sp * tp + c) for i in range(sp) for c in range(tp)]
    against = [(b, a) for a, b in along]
    sign = 1 - 2 * side
    width = x.shape[1] // parts
    start = [x[:, p * width : (p + 1) * width] for p in range(parts)]
    ahead, behind = list(start), list(start)
    pieces, order = [start], [here]
    for s in range(1, sp // 2 + 1):
        both = s < sp - sp // 2
        ahead = [lax.ppermute(a, ("sp", "tp"), along) for a in ahead]
        if both:
            behind = [lax.ppermute(a, ("sp", "tp"), against) for a in behind]
            for p in range(parts):
                ahead[p], behind[p] = lax.optimization_barrier((ahead[p], behind[p]))
        pieces.append(list(ahead))
        order.append((here - sign * s) % sp)
        if both:
            pieces.append(list(behind))
            order.append((here + sign * s) % sp)
    return [p for block in pieces for p in block], jnp.stack(order)


def body(
    tokens,
    norm_gain,
    w_z,
    w_x,
    w_b,
    w_c,
    w_dt,
    w_gate,
    w_scb,
    w_scc,
    w_scx,
    conv_x,
    conv_b,
    conv_c,
    conv_sc,
    dt_bias,
    decay_log,
    group_gain,
    span_shift,
    w_out,
):
    sp, fs, tp = (lax.axis_size(a) for a in ("sp", "fs", "tp"))
    here, side, fs_here = (lax.axis_index(a) for a in ("sp", "tp", "fs"))
    own = tokens[0]
    length, half = own.shape
    hd = HEAD_DIM
    heads = dt_bias.shape[0]
    share = heads // sp
    groups = conv_b.shape[1] // hd
    per_group = heads // groups
    depth = w_x.shape[0]

    payload = jnp.concatenate([own, w_out], axis=0)
    parts = 2
    pieces, order = ring(payload, parts)
    swap = [(i, tp - 1 - i) for i in range(tp)]
    partner = lax.ppermute(own, "tp", swap)
    rows = jnp.where(
        side == 0, jnp.concatenate([own, partner], axis=1), jnp.concatenate([partner, own], axis=1)
    ).astype(F32)
    inverse_rms = lax.rsqrt(jnp.mean(rows * rows, axis=1, keepdims=True) + EPS)
    normed = (rows * inverse_rms * norm_gain).astype(BF16)
    narrow = jnp.concatenate([w_dt, w_gate.reshape(w_gate.shape[0], -1)], axis=1)
    small = dot(narrow, normed, ((0,), (1,)))
    shift = jnp.repeat(span_shift[0], BLOCK)
    step = jax.nn.softplus(small[:heads] + dt_bias[:, None] + shift[None, :])
    rate = -jnp.exp(decay_log)[:, None]
    upper = (lax.iota(jnp.int32, length)[:, None] <= lax.iota(jnp.int32, length)[None, :]).astype(F32)
    cum = jnp.dot(step * rate, upper, precision=HIGH)
    gates = jax.nn.sigmoid(small[heads:])
    inverse_rows = jnp.broadcast_to(inverse_rms[:, 0][None, :], (heads, length))
    info = jnp.stack([step, cum, gates[:heads], gates[heads:], inverse_rows], axis=1)
    info = jnp.pad(info, ((0, 0), (0, EDGE - info.shape[1]), (0, 0)))
    row_gain = lax.dynamic_slice_in_dim(norm_gain, (here * fs + fs_here) * depth, depth)[:, None]
    packed = pl.pallas_call(
        functools.partial(pack_kernel, per_group),
        out_shape=jax.ShapeDtypeStruct((sp, depth + EDGE, 8 * hd), BF16),
        name="pack",
    )(row_gain, info, w_x, w_b, w_c, w_z, w_scc, w_scb, w_scx)
    cols = packed.shape[2]
    got = lax.all_to_all(packed, "sp", 0, 0, tiled=True)
    hold = (HOLD * 2 - 1) * parts
    got, *pieces[hold : hold + parts] = lax.optimization_barrier((got, *pieces[hold : hold + parts]))
    info = sum(got[:, depth:, k * length : (k + 1) * length].astype(F32) for k in range(3))
    halves = got[:, :depth].reshape(tp, (sp // tp) * depth, cols)
    halves = jnp.broadcast_to(halves, (fs, *halves.shape)).reshape(fs * tp, -1, cols)
    halves = lax.all_to_all(halves, ("fs", "tp"), 0, 0, tiled=True).reshape(fs, tp, sp // tp, depth, cols)

    def head_of(a, dim):
        return lax.dynamic_slice_in_dim(a, here * share * hd, share * hd, dim)

    def group_of(a):
        return lax.dynamic_slice_in_dim(a, (here * share // per_group) * hd, hd, 1)

    taps = jnp.concatenate([head_of(conv_x, 1), group_of(conv_b), group_of(conv_c)], axis=1)
    taps = jnp.pad(taps, ((0, 0), (0, hd)))
    taps_sc = head_of(conv_sc, 1)
    own_gain = head_of(group_gain, 0)[None]
    halves, info, taps, taps_sc, own_gain = lax.optimization_barrier((halves, info, taps, taps_sc, own_gain))

    def w_rows_of(lo, hi):
        blocks = [jnp.concatenate([p[length:] for p in pieces[k * parts : (k + 1) * parts]], axis=1) for k in range(lo, hi)]
        return jnp.stack(blocks)

    def moved(rows):
        found = [rows]
        for k in range(1, fs):
            found.append(lax.ppermute(rows, "fs", [(i, (i + k) % fs) for i in range(fs)]))
        return found

    cut = 1 + 2 * HOLD
    early = moved(w_rows_of(0, cut))
    late = moved(w_rows_of(cut, sp))

    vmem = pl.BlockSpec(memory_space=pltpu.VMEM)
    smem = pl.BlockSpec(memory_space=pltpu.SMEM)
    project = pl.pallas_call(
        functools.partial(project_kernel, sp, parts, sp // 2 * length, 256),
        in_specs=[smem] * 2 + [vmem] * (len(pieces) + 1),
        out_specs=vmem,
        out_shape=jax.ShapeDtypeStruct((sp, length, cols), BF16),
        scratch_shapes=[pltpu.VMEM((sp * length, half), BF16), pltpu.VMEM((half, cols), BF16)],
        name="project",
    )
    other = project(order, (tp - 1 - side)[None], *pieces, halves)
    arrived = lax.ppermute(other, "tp", swap)
    mine = project(order, side[None], *pieces, halves)

    many = 2
    block = lambda shape: pl.BlockSpec((many, *shape), lambda i: (i,) + (0,) * len(shape))
    whole = lambda a: pl.BlockSpec(a.shape, lambda i: (0,) * a.ndim)
    mixer = pl.pallas_call(
        functools.partial(mixer_kernel, many, taps.shape[0], taps_sc.shape[0]),
        grid=(sp // many,),
        in_specs=[
            block((length, cols)),
            block((length, cols)),
            block((EDGE, length)),
            whole(taps),
            whole(taps_sc),
            whole(own_gain),
        ],
        out_specs=block((length + EDGE, 2 * hd)),
        out_shape=jax.ShapeDtypeStruct((sp, length + EDGE, 2 * hd), BF16),
        scratch_shapes=[pltpu.VMEM((EDGE, 6 * hd), F32), pltpu.VMEM((hd, hd), F32)],
        name="mixer",
    )
    ab = mixer(mine, arrived, info, taps, taps_sc, own_gain)

    place = jnp.stack([(fs_here - k) % fs for k in range(fs)])
    w_all = pl.pallas_call(
        assemble_kernel,
        in_specs=[smem] * 2 + [vmem] * (2 * fs),
        out_specs=vmem,
        out_shape=jax.ShapeDtypeStruct((sp * fs * depth, half), BF16),
        name="assemble",
    )(order, place, *early, *late)

    ab = lax.all_to_all(ab, "sp", 0, 0, tiled=True)
    merged = pl.pallas_call(
        functools.partial(merge_kernel, per_group),
        out_shape=jax.ShapeDtypeStruct((length, sp * hd), BF16),
        name="merge",
    )(ab)
    partial = dot(merged, w_all, ((1,), (1,))).astype(BF16)
    parts = partial.reshape(tp, length // tp, partial.shape[1])
    parts = lax.all_to_all(parts, "tp", 0, 0, tiled=True)
    return parts.astype(F32).sum(axis=0).astype(BF16)[None]


def solution(mesh):
    return mapped(mesh)


def mapped(mesh):
    return jax.shard_map(
        body,
        mesh=mesh,
        in_specs=(
            P(("grp", "fs"), "sp", "tp"),
            P(),
            P(("sp", "fs"), "tp"),
            P(("sp", "fs"), "tp"),
            P(("sp", "fs"), "tp"),
            P(("sp", "fs"), "tp"),
            P(None, "tp"),
            P(None, None, "tp"),
            P(("sp", "fs"), "tp"),
            P(("sp", "fs"), "tp"),
            P(("sp", "fs"), "tp"),
            P(None, "tp"),
            P(None, "tp"),
            P(None, "tp"),
            P(None, "tp"),
            P("tp"),
            P("tp"),
            P("tp"),
            P(("grp", "fs"), "sp"),
            P(("sp", "fs"), "tp"),
        ),
        out_specs=P(("grp", "fs"), ("sp", "tp"), None),
        check_vma=False,
    )
```

```python
import functools

import jax
import jax.numpy as jnp
from jax import lax
from jax.experimental import pallas as pl
from jax.experimental.pallas import tpu as pltpu
from jax.sharding import PartitionSpec as P


HEAD_DIM = 64
BLOCK = 64
EDGE = 8
HOLD = 4
EPS = 1.0
HIGH = lax.Precision.HIGHEST
F32 = jnp.float32
BF16 = jnp.bfloat16


def silu(v):
    return v / (1.0 + jnp.exp(-v))


def dot(a, b, contract=((1,), (0,))):
    return lax.dot_general(a, b, (contract, ((), ())), preferred_element_type=F32)


def taps_of(extended, taps_ref, count, length):
    first = EDGE - count + 1
    result = extended[first : first + length] * taps_ref[0:1]
    for k in range(1, count):
        result = result + extended[first + k : first + k + length] * taps_ref[k : k + 1]
    return result


def mixer_kernel(
    many, long_taps, short_taps, own_ref, recv_ref, rows_ref, taps_ref, taps_sc_ref, gain_ref, ab_ref, square_ref, tail_ref, state_ref
):
    length = ab_ref.shape[1]
    hd = HEAD_DIM

    @pl.when(pl.program_id(0) == 0)
    def _():
        tail_ref[...] = jnp.zeros_like(tail_ref)
        state_ref[...] = jnp.zeros_like(state_ref)

    lower = lax.broadcasted_iota(jnp.int32, (length, length), 0) >= lax.broadcasted_iota(
        jnp.int32, (length, length), 1
    )
    tail = tail_ref[...]
    state = state_ref[...]
    for k in range(many):
        rows = rows_ref[k]
        cols = rows.T
        step, cum, gate, gate_sc, inverse = (cols[:, i : i + 1] for i in range(5))
        stream = (own_ref[k].astype(F32) + recv_ref[k].astype(F32)) * inverse
        short_in = stream[:, 4 * hd : 5 * hd] * stream[:, 6 * hd : 7 * hd]
        conv = taps_of(jnp.concatenate([tail[:, : 4 * hd], stream[:, : 4 * hd]], axis=0), taps_ref, long_taps, length)
        conv_sc = taps_of(
            jnp.concatenate([tail[:, 4 * hd : 5 * hd], short_in], axis=0), taps_sc_ref, short_taps, length
        )
        tail = jnp.concatenate([stream[length - EDGE :, : 4 * hd], short_in[length - EDGE :], short_in[length - EDGE :]], axis=1)
        conv = silu(conv[:, : 3 * hd])
        x = conv[:, :hd] * step
        b = conv[:, hd : 2 * hd].astype(BF16)
        c = conv[:, 2 * hd : 3 * hd]
        z = stream[:, 3 * hd : 4 * hd]
        scb = stream[:, 5 * hd : 6 * hd]
        scores = dot(c.astype(BF16), b, ((1,), (1,)))
        decay = jnp.where(lower, jnp.exp(jnp.minimum(cum - rows[1:2], 0.0)), 0.0)
        core = dot((scores * decay).astype(BF16), x.astype(BF16))
        core = core + dot((c * jnp.exp(cum)).astype(BF16), state.astype(BF16), ((1,), (1,)))
        last = cum[length - 1 : length]
        fresh = dot((x * jnp.exp(last - cum)).astype(BF16), b, ((0,), (0,)))
        state = state * jnp.exp(last) + fresh
        gated = core * silu(z)
        square_ref[k] = lax.dot_general(
            jnp.ones((EDGE, hd), F32), gated * gated, (((1,), (1,)), ((), ())), precision=HIGH, preferred_element_type=F32
        )
        both = jnp.concatenate([gated * gain_ref[...] * gate, gate_sc * (scb * conv_sc)], axis=1)
        ab_ref[k] = both.astype(BF16)
    tail_ref[...] = tail
    state_ref[...] = state


def merge_kernel(per_group, ab_ref, squares_ref, out_ref):
    hd = HEAD_DIM
    total = squares_ref[0]
    for k in range(1, per_group):
        total = total + squares_ref[k]
    scale = lax.rsqrt(total * (1.0 / (per_group * hd)) + EPS).T
    half = out_ref.shape[1]
    for k in range(out_ref.shape[0]):
        ab = ab_ref[k].astype(F32)
        merged = (ab[:, :hd] * scale[:, k : k + 1] + ab[:, hd:]).astype(BF16)
        out_ref[k] = jnp.concatenate([merged[:half], merged[half:]], axis=1)


def output_kernel(tile, merged_ref, w_ref, out_ref, left_ref):
    count, half, _ = merged_ref.shape
    hd = HEAD_DIM
    for k in range(0, count, 2):
        first, second = merged_ref[k], merged_ref[k + 1]
        lanes = slice(k * hd, (k + 2) * hd)
        left_ref[:half, lanes] = jnp.concatenate([first[:, :hd], second[:, :hd]], axis=1)
        left_ref[half:, lanes] = jnp.concatenate([first[:, hd:], second[:, hd:]], axis=1)
    left = left_ref[...]
    for lo in range(0, out_ref.shape[1], tile):
        out_ref[:, lo : lo + tile] = dot(left, w_ref[lo : lo + tile, :], ((1,), (1,))).astype(BF16)


def rows_kernel(parts, *refs):
    out_ref = refs[-1]
    width = refs[0].shape[1]
    for k in range(out_ref.shape[0]):
        for p in range(parts):
            out_ref[k, :, p * width : (p + 1) * width] = refs[k * parts + p][...]


def pack_kernel(per_group, gain_ref, info_ref, x_ref, b_ref, c_ref, z_ref, scc_ref, scb_ref, scx_ref, out_ref):
    hd = HEAD_DIM
    depth = x_ref.shape[0]
    gain = gain_ref[...]
    scaled = [(ref[...].astype(F32) * gain).astype(BF16) for ref in (x_ref, b_ref, c_ref, z_ref, scc_ref, scb_ref, scx_ref)]
    x, b, c, z, scc, scb, scx = scaled
    for h in range(out_ref.shape[0]):
        g = h // per_group
        own = slice(h * hd, (h + 1) * hd)
        group = slice(g * hd, (g + 1) * hd)
        parts = [x[:, own], b[:, group], c[:, group], z[:, own], scc[:, own], scb[:, own], scx[:, own]]
        parts += [jnp.zeros_like(parts[0])]
        out_ref[h, :depth, :] = jnp.concatenate(parts, axis=1)
        left = info_ref[h]
        split = []
        for _ in range(3):
            part = left.astype(BF16)
            split.append(part)
            left = left - part.astype(F32)
        split.append(jnp.zeros_like(split[0]))
        out_ref[h, depth:, :] = jnp.concatenate(split, axis=1)


def project_kernel(count, parts, rows, tile, order_ref, source_ref, *refs):
    pieces = refs[: count * parts]
    halves_ref, out_ref, tokens_ref, w_ref = refs[count * parts :]
    length, cols = out_ref.shape[1:]
    width = pieces[0].shape[1]
    fs, _, spans, depth, _ = halves_ref.shape
    source = source_ref[0]
    for k in range(count):
        at = pl.multiple_of(order_ref[k] * length, length)
        for p in range(parts):
            tokens_ref[pl.ds(at, length), p * width : (p + 1) * width] = pieces[k * parts + p][:length, :]
    for span in range(spans):
        for f in range(fs):
            lo = (span * fs + f) * depth
            w_ref[lo : lo + depth, :] = halves_ref[f, source, span]

    @pl.loop(0, count * length // rows)
    def _(step):
        left = tokens_ref[pl.ds(pl.multiple_of(step * rows, rows), rows), :]
        for lo in range(0, cols, tile):
            total = dot(left, w_ref[:, lo : lo + tile]).astype(BF16)
            out_ref[pl.ds(step * (rows // length), rows // length), :, lo : lo + tile] = total.reshape(
                rows // length, length, tile
            )


def assemble_kernel(order_ref, place_ref, *refs):
    early, late, out_ref = refs[: (len(refs) - 1) // 2], refs[(len(refs) - 1) // 2 : -1], refs[-1]
    first, depth = early[0].shape[:2]
    for k in range(len(early)):
        for ref, base in ((early[k], 0), (late[k], first)):
            for j in range(ref.shape[0]):
                at = pl.multiple_of((order_ref[base + j] * len(early) + place_ref[k]) * depth, depth)
                out_ref[pl.ds(at, depth), :] = ref[j]


def ring(x, parts):
    sp, tp = lax.axis_size("sp"), lax.axis_size("tp")
    here, side = lax.axis_index("sp"), lax.axis_index("tp")
    along = [(i * tp + c, (i + 1 - 2 * c) % sp * tp + c) for i in range(sp) for c in range(tp)]
    against = [(b, a) for a, b in along]
    sign = 1 - 2 * side
    width = x.shape[1] // parts
    start = [x[:, p * width : (p + 1) * width] for p in range(parts)]
    ahead, behind = list(start), list(start)
    pieces, order = [start], [here]
    for s in range(1, sp // 2 + 1):
        both = s < sp - sp // 2
        ahead = [lax.ppermute(a, ("sp", "tp"), along) for a in ahead]
        if both:
            behind = [lax.ppermute(a, ("sp", "tp"), against) for a in behind]
            for p in range(parts):
                ahead[p], behind[p] = lax.optimization_barrier((ahead[p], behind[p]))
        pieces.append(list(ahead))
        order.append((here - sign * s) % sp)
        if both:
            pieces.append(list(behind))
            order.append((here + sign * s) % sp)
    return [p for block in pieces for p in block], jnp.stack(order)


def body(
    tokens,
    norm_gain,
    w_z,
    w_x,
    w_b,
    w_c,
    w_dt,
    w_gate,
    w_scb,
    w_scc,
    w_scx,
    conv_x,
    conv_b,
    conv_c,
    conv_sc,
    dt_bias,
    decay_log,
    group_gain,
    span_shift,
    w_out,
):
    sp, fs, tp = (lax.axis_size(a) for a in ("sp", "fs", "tp"))
    here, side, fs_here = (lax.axis_index(a) for a in ("sp", "tp", "fs"))
    own = tokens[0]
    length, half = own.shape
    hd = HEAD_DIM
    heads = dt_bias.shape[0]
    share = heads // sp
    groups = conv_b.shape[1] // hd
    per_group = heads // groups
    depth = w_x.shape[0]

    payload = jnp.concatenate([own, w_out], axis=0)
    parts = 2
    pieces, order = ring(payload, parts)
    swap = [(i, tp - 1 - i) for i in range(tp)]
    partner = lax.ppermute(own, "tp", swap)
    rows = jnp.where(
        side == 0, jnp.concatenate([own, partner], axis=1), jnp.concatenate([partner, own], axis=1)
    ).astype(F32)
    inverse_rms = lax.rsqrt(jnp.mean(rows * rows, axis=1, keepdims=True) + EPS)
    normed = (rows * inverse_rms * norm_gain).astype(BF16)
    narrow = jnp.concatenate([w_dt, w_gate.reshape(w_gate.shape[0], -1)], axis=1)
    small = dot(narrow, normed, ((0,), (1,)))
    shift = jnp.repeat(span_shift[0], BLOCK)
    step = jax.nn.softplus(small[:heads] + dt_bias[:, None] + shift[None, :])
    rate = -jnp.exp(decay_log)[:, None]
    upper = (lax.iota(jnp.int32, length)[:, None] <= lax.iota(jnp.int32, length)[None, :]).astype(F32)
    cum = jnp.dot(step * rate, upper, precision=HIGH)
    gates = jax.nn.sigmoid(small[heads:])
    inverse_rows = jnp.broadcast_to(inverse_rms[:, 0][None, :], (heads, length))
    info = jnp.stack([step, cum, gates[:heads], gates[heads:], inverse_rows], axis=1)
    info = jnp.pad(info, ((0, 0), (0, EDGE - info.shape[1]), (0, 0)))
    row_gain = lax.dynamic_slice_in_dim(norm_gain, (here * fs + fs_here) * depth, depth)[:, None]
    packed = pl.pallas_call(
        functools.partial(pack_kernel, per_group),
        out_shape=jax.ShapeDtypeStruct((sp, depth + EDGE, 8 * hd), BF16),
        name="pack",
    )
    packed = packed(row_gain, info, w_x, w_b, w_c, w_z, w_scc, w_scb, w_scx)
    cols = packed.shape[2]
    got = lax.all_to_all(packed, "sp", 0, 0, tiled=True)
    hold = (HOLD * 2 - 1) * parts
    got, *pieces[hold : hold + parts] = lax.optimization_barrier((got, *pieces[hold : hold + parts]))
    info = sum(got[:, depth:, k * length : (k + 1) * length].astype(F32) for k in range(3))
    halves = got[:, :depth].reshape(tp, (sp // tp) * depth, cols)
    halves = jnp.broadcast_to(halves, (fs, *halves.shape)).reshape(fs * tp, -1, cols)
    halves = lax.all_to_all(halves, ("fs", "tp"), 0, 0, tiled=True).reshape(fs, tp, sp // tp, depth, cols)

    def head_of(a, dim):
        return lax.dynamic_slice_in_dim(a, here * share * hd, share * hd, dim)

    def group_of(a):
        return lax.dynamic_slice_in_dim(a, (here * share // per_group) * hd, hd, 1)

    taps = jnp.concatenate([head_of(conv_x, 1), group_of(conv_b), group_of(conv_c)], axis=1)
    taps = jnp.pad(taps, ((0, 0), (0, hd)))
    taps_sc = head_of(conv_sc, 1)
    own_gain = head_of(group_gain, 0)[None]
    halves, info, taps, taps_sc, own_gain = lax.optimization_barrier((halves, info, taps, taps_sc, own_gain))

    def w_rows_of(lo, hi):
        some = pieces[lo * parts : hi * parts]
        return pl.pallas_call(
            functools.partial(rows_kernel, parts),
            grid=(1,),
            in_specs=[pl.BlockSpec((depth, half // parts), lambda i: (length // depth, 0))] * len(some),
            out_specs=pl.BlockSpec((hi - lo, depth, half), lambda i: (0, 0, 0)),
            out_shape=jax.ShapeDtypeStruct((hi - lo, depth, half), BF16),
            name="rows",
        )(*some)

    def moved(rows):
        found = [rows]
        for k in range(1, fs):
            found.append(lax.ppermute(rows, "fs", [(i, (i + k) % fs) for i in range(fs)]))
        return found

    cut = 1 + 2 * HOLD
    early = moved(w_rows_of(0, cut))
    late = moved(w_rows_of(cut, sp))

    vmem = pl.BlockSpec(memory_space=pltpu.VMEM)
    smem = pl.BlockSpec(memory_space=pltpu.SMEM)
    project = pl.pallas_call(
        functools.partial(project_kernel, sp, parts, sp // 2 * length, 256),
        in_specs=[smem] * 2 + [vmem] * (len(pieces) + 1),
        out_specs=vmem,
        out_shape=jax.ShapeDtypeStruct((sp, length, cols), BF16),
        scratch_shapes=[pltpu.VMEM((sp * length, half), BF16), pltpu.VMEM((half, cols), BF16)],
        name="project",
    )
    other = project(order, (tp - 1 - side)[None], *pieces, halves)
    arrived = lax.ppermute(other, "tp", swap)
    mine = project(order, side[None], *pieces, halves)

    many = 2
    block = lambda shape: pl.BlockSpec((many, *shape), lambda i: (i,) + (0,) * len(shape))
    whole = lambda a: pl.BlockSpec(a.shape, lambda i: (0,) * a.ndim)
    mixer = pl.pallas_call(
        functools.partial(mixer_kernel, many, taps.shape[0], taps_sc.shape[0]),
        grid=(sp // many,),
        in_specs=[
            block((length, cols)),
            block((length, cols)),
            block((EDGE, length)),
            whole(taps),
            whole(taps_sc),
            whole(own_gain),
        ],
        out_specs=[block((length, 2 * hd)), block((EDGE, length))],
        out_shape=[
            jax.ShapeDtypeStruct((sp, length, 2 * hd), BF16),
            jax.ShapeDtypeStruct((sp, EDGE, length), F32),
        ],
        scratch_shapes=[pltpu.VMEM((EDGE, 6 * hd), F32), pltpu.VMEM((hd, hd), F32)],
        name="mixer",
    )
    ab, squares = mixer(mine, arrived, info, taps, taps_sc, own_gain)

    place = jnp.stack([(fs_here - k) % fs for k in range(fs)])
    w_all = pl.pallas_call(
        assemble_kernel,
        in_specs=[smem] * 2 + [vmem] * (2 * fs),
        out_specs=vmem,
        out_shape=jax.ShapeDtypeStruct((sp * fs * depth, half), BF16),
        name="assemble",
    )(order, place, *early, *late)

    squares = jnp.broadcast_to(squares[:, 0], (per_group, sp, length))
    neighbours = [[g * per_group + k for k in range(per_group)] for g in range(groups)]
    squares = lax.all_to_all(squares, "sp", 0, 0, tiled=True, axis_index_groups=neighbours)
    merged = pl.pallas_call(
        functools.partial(merge_kernel, per_group),
        out_shape=jax.ShapeDtypeStruct((sp, length // 2, 2 * hd), BF16),
        name="merge",
    )(ab, squares)
    merged = lax.all_to_all(merged, "sp", 0, 0, tiled=True)
    partial = pl.pallas_call(
        functools.partial(output_kernel, 512),
        out_shape=jax.ShapeDtypeStruct((length, w_all.shape[0]), BF16),
        scratch_shapes=[pltpu.VMEM((length, half), BF16)],
        name="output",
    )(merged, w_all)
    parts = partial.reshape(tp, length // tp, partial.shape[1])
    parts = lax.all_to_all(parts, "tp", 0, 0, tiled=True)
    return parts.astype(F32).sum(axis=0).astype(BF16)[None]


def solution(mesh):
    return mapped(mesh)


def mapped(mesh):
    return jax.shard_map(
        body,
        mesh=mesh,
        in_specs=(
            P(("grp", "fs"), "sp", "tp"),
            P(),
            P(("sp", "fs"), "tp"),
            P(("sp", "fs"), "tp"),
            P(("sp", "fs"), "tp"),
            P(("sp", "fs"), "tp"),
            P(None, "tp"),
            P(None, None, "tp"),
            P(("sp", "fs"), "tp"),
            P(("sp", "fs"), "tp"),
            P(("sp", "fs"), "tp"),
            P(None, "tp"),
            P(None, "tp"),
            P(None, "tp"),
            P(None, "tp"),
            P("tp"),
            P("tp"),
            P("tp"),
            P(("grp", "fs"), "sp"),
            P(("sp", "fs"), "tp"),
        ),
        out_specs=P(("grp", "fs"), ("sp", "tp"), None),
        check_vma=False,
    )
```

```python
import functools

import jax
import jax.numpy as jnp
from jax import lax
from jax.experimental import pallas as pl
from jax.experimental.pallas import tpu as pltpu
from jax.sharding import PartitionSpec as P


HEAD_DIM = 64
BLOCK = 64
EDGE = 8
HOLD = 4
EPS = 1.0
HIGH = lax.Precision.HIGHEST
F32 = jnp.float32
BF16 = jnp.bfloat16


def silu(v):
    return v / (1.0 + jnp.exp(-v))


def dot(a, b, contract=((1,), (0,))):
    return lax.dot_general(a, b, (contract, ((), ())), preferred_element_type=F32)


def taps_of(extended, taps_ref, count, length):
    first = EDGE - count + 1
    result = extended[first : first + length] * taps_ref[0:1]
    for k in range(1, count):
        result = result + extended[first + k : first + k + length] * taps_ref[k : k + 1]
    return result


def mixer_kernel(
    many, long_taps, short_taps, own_ref, recv_ref, rows_ref, taps_ref, taps_sc_ref, gain_ref, ab_ref, square_ref, tail_ref, state_ref
):
    length = ab_ref.shape[1]
    hd = HEAD_DIM

    @pl.when(pl.program_id(0) == 0)
    def _():
        tail_ref[...] = jnp.zeros_like(tail_ref)
        state_ref[...] = jnp.zeros_like(state_ref)

    lower = lax.broadcasted_iota(jnp.int32, (length, length), 0) >= lax.broadcasted_iota(
        jnp.int32, (length, length), 1
    )
    tail = tail_ref[...]
    state = state_ref[...]
    for k in range(many):
        rows = rows_ref[k]
        cols = rows.T
        step, cum, gate, gate_sc, inverse = (cols[:, i : i + 1] for i in range(5))
        stream = (own_ref[k].astype(F32) + recv_ref[k].astype(F32)) * inverse
        short_in = stream[:, 4 * hd : 5 * hd] * stream[:, 6 * hd : 7 * hd]
        conv = taps_of(jnp.concatenate([tail[:, : 4 * hd], stream[:, : 4 * hd]], axis=0), taps_ref, long_taps, length)
        conv_sc = taps_of(
            jnp.concatenate([tail[:, 4 * hd : 5 * hd], short_in], axis=0), taps_sc_ref, short_taps, length
        )
        tail = jnp.concatenate([stream[length - EDGE :, : 4 * hd], short_in[length - EDGE :], short_in[length - EDGE :]], axis=1)
        conv = silu(conv[:, : 3 * hd])
        x = conv[:, :hd] * step
        b = conv[:, hd : 2 * hd].astype(BF16)
        c = conv[:, 2 * hd : 3 * hd]
        z = stream[:, 3 * hd : 4 * hd]
        scb = stream[:, 5 * hd : 6 * hd]
        scores = dot(c.astype(BF16), b, ((1,), (1,)))
        decay = jnp.where(lower, jnp.exp(jnp.minimum(cum - rows[1:2], 0.0)), 0.0)
        core = dot((scores * decay).astype(BF16), x.astype(BF16))
        core = core + dot((c * jnp.exp(cum)).astype(BF16), state.astype(BF16), ((1,), (1,)))
        last = cum[length - 1 : length]
        fresh = dot((x * jnp.exp(last - cum)).astype(BF16), b, ((0,), (0,)))
        state = state * jnp.exp(last) + fresh
        gated = core * silu(z)
        square_ref[k] = lax.dot_general(
            jnp.ones((EDGE, hd), F32), gated * gated, (((1,), (1,)), ((), ())), precision=HIGH, preferred_element_type=F32
        )
        both = jnp.concatenate([gated * gain_ref[...] * gate, gate_sc * (scb * conv_sc)], axis=1)
        ab_ref[k] = both.astype(BF16)
    tail_ref[...] = tail
    state_ref[...] = state


def merge_kernel(per_group, ab_ref, squares_ref, out_ref):
    hd = HEAD_DIM
    total = squares_ref[0]
    for k in range(1, per_group):
        total = total + squares_ref[k]
    scale = lax.rsqrt(total * (1.0 / (per_group * hd)) + EPS).T
    half = out_ref.shape[1]
    for k in range(out_ref.shape[0]):
        ab = ab_ref[k].astype(F32)
        merged = (ab[:, :hd] * scale[:, k : k + 1] + ab[:, hd:]).astype(BF16)
        out_ref[k] = jnp.concatenate([merged[:half], merged[half:]], axis=1)


def output_kernel(tile, merged_ref, w_ref, out_ref, left_ref):
    count, half, _ = merged_ref.shape
    hd = HEAD_DIM
    for k in range(0, count, 2):
        first, second = merged_ref[k], merged_ref[k + 1]
        lanes = slice(k * hd, (k + 2) * hd)
        left_ref[:half, lanes] = jnp.concatenate([first[:, :hd], second[:, :hd]], axis=1)
        left_ref[half:, lanes] = jnp.concatenate([first[:, hd:], second[:, hd:]], axis=1)
    left = left_ref[...]
    for lo in range(0, out_ref.shape[1], tile):
        out_ref[:, lo : lo + tile] = dot(left, w_ref[lo : lo + tile, :], ((1,), (1,))).astype(BF16)


def rows_kernel(parts, *refs):
    out_ref = refs[-1]
    width = refs[0].shape[1]
    for k in range(out_ref.shape[0]):
        for p in range(parts):
            out_ref[k, :, p * width : (p + 1) * width] = refs[k * parts + p][...]


def pack_kernel(per_group, gain_ref, info_ref, x_ref, b_ref, c_ref, z_ref, scc_ref, scb_ref, scx_ref, out_ref):
    hd = HEAD_DIM
    depth = x_ref.shape[0]
    gain = gain_ref[...]
    scaled = [(ref[...].astype(F32) * gain).astype(BF16) for ref in (x_ref, b_ref, c_ref, z_ref, scc_ref, scb_ref, scx_ref)]
    x, b, c, z, scc, scb, scx = scaled
    for h in range(out_ref.shape[0]):
        g = h // per_group
        own = slice(h * hd, (h + 1) * hd)
        group = slice(g * hd, (g + 1) * hd)
        parts = [x[:, own], b[:, group], c[:, group], z[:, own], scc[:, own], scb[:, own], scx[:, own]]
        parts += [jnp.zeros_like(parts[0])]
        out_ref[h, :depth, :] = jnp.concatenate(parts, axis=1)
        left = info_ref[h]
        split = []
        for _ in range(3):
            part = left.astype(BF16)
            split.append(part)
            left = left - part.astype(F32)
        split.append(jnp.zeros_like(split[0]))
        out_ref[h, depth:, :] = jnp.concatenate(split, axis=1)


def project_kernel(count, parts, rows, tile, order_ref, source_ref, *refs):
    pieces = refs[: count * parts]
    halves_ref, out_ref, tokens_ref, w_ref = refs[count * parts :]
    length, cols = out_ref.shape[1:]
    width = pieces[0].shape[1]
    fs, _, spans, depth, _ = halves_ref.shape
    source = source_ref[0]
    for k in range(count):
        at = pl.multiple_of(order_ref[k] * length, length)
        for p in range(parts):
            tokens_ref[pl.ds(at, length), p * width : (p + 1) * width] = pieces[k * parts + p][:length, :]
    for span in range(spans):
        for f in range(fs):
            lo = (span * fs + f) * depth
            w_ref[lo : lo + depth, :] = halves_ref[f, source, span]

    @pl.loop(0, count * length // rows)
    def _(step):
        left = tokens_ref[pl.ds(pl.multiple_of(step * rows, rows), rows), :]
        for lo in range(0, cols, tile):
            total = dot(left, w_ref[:, lo : lo + tile]).astype(BF16)
            out_ref[pl.ds(step * (rows // length), rows // length), :, lo : lo + tile] = total.reshape(
                rows // length, length, tile
            )


def assemble_kernel(order_ref, place_ref, *refs):
    early, late, out_ref = refs[: (len(refs) - 1) // 2], refs[(len(refs) - 1) // 2 : -1], refs[-1]
    first, depth = early[0].shape[:2]
    for k in range(len(early)):
        for ref, base in ((early[k], 0), (late[k], first)):
            for j in range(ref.shape[0]):
                at = pl.multiple_of((order_ref[base + j] * len(early) + place_ref[k]) * depth, depth)
                out_ref[pl.ds(at, depth), :] = ref[j]


def ring(x, parts):
    sp, tp = lax.axis_size("sp"), lax.axis_size("tp")
    here, side = lax.axis_index("sp"), lax.axis_index("tp")
    along = [(i * tp + c, (i + 1 - 2 * c) % sp * tp + c) for i in range(sp) for c in range(tp)]
    against = [(b, a) for a, b in along]
    sign = 1 - 2 * side
    width = x.shape[1] // parts
    start = [x[:, p * width : (p + 1) * width] for p in range(parts)]
    ahead, behind = list(start), list(start)
    pieces, order = [start], [here]
    for s in range(1, sp // 2 + 1):
        both = s < sp - sp // 2
        for p in range(parts):
            ahead[p] = lax.ppermute(ahead[p], ("sp", "tp"), along)
            if both:
                behind[p] = lax.ppermute(behind[p], ("sp", "tp"), against)
        pieces.append(list(ahead))
        order.append((here - sign * s) % sp)
        if both:
            pieces.append(list(behind))
            order.append((here + sign * s) % sp)
    return [p for block in pieces for p in block], jnp.stack(order)


def body(
    tokens,
    norm_gain,
    w_z,
    w_x,
    w_b,
    w_c,
    w_dt,
    w_gate,
    w_scb,
    w_scc,
    w_scx,
    conv_x,
    conv_b,
    conv_c,
    conv_sc,
    dt_bias,
    decay_log,
    group_gain,
    span_shift,
    w_out,
):
    sp, fs, tp = (lax.axis_size(a) for a in ("sp", "fs", "tp"))
    here, side, fs_here = (lax.axis_index(a) for a in ("sp", "tp", "fs"))
    own = tokens[0]
    length, half = own.shape
    hd = HEAD_DIM
    heads = dt_bias.shape[0]
    share = heads // sp
    groups = conv_b.shape[1] // hd
    per_group = heads // groups
    depth = w_x.shape[0]

    payload = jnp.concatenate([own, w_out], axis=0)
    parts = 2
    pieces, order = ring(payload, parts)
    swap = [(i, tp - 1 - i) for i in range(tp)]
    partner = lax.ppermute(own, "tp", swap)
    rows = jnp.where(
        side == 0, jnp.concatenate([own, partner], axis=1), jnp.concatenate([partner, own], axis=1)
    ).astype(F32)
    inverse_rms = lax.rsqrt(jnp.mean(rows * rows, axis=1, keepdims=True) + EPS)
    normed = (rows * inverse_rms * norm_gain).astype(BF16)
    narrow = jnp.concatenate([w_dt, w_gate.reshape(w_gate.shape[0], -1)], axis=1)
    small = dot(narrow, normed, ((0,), (1,)))
    shift = jnp.repeat(span_shift[0], BLOCK)
    step = jax.nn.softplus(small[:heads] + dt_bias[:, None] + shift[None, :])
    rate = -jnp.exp(decay_log)[:, None]
    upper = (lax.iota(jnp.int32, length)[:, None] <= lax.iota(jnp.int32, length)[None, :]).astype(F32)
    cum = jnp.dot(step * rate, upper, precision=HIGH)
    gates = jax.nn.sigmoid(small[heads:])
    inverse_rows = jnp.broadcast_to(inverse_rms[:, 0][None, :], (heads, length))
    info = jnp.stack([step, cum, gates[:heads], gates[heads:], inverse_rows], axis=1)
    info = jnp.pad(info, ((0, 0), (0, EDGE - info.shape[1]), (0, 0)))
    row_gain = lax.dynamic_slice_in_dim(norm_gain, (here * fs + fs_here) * depth, depth)[:, None]
    packed = pl.pallas_call(
        functools.partial(pack_kernel, per_group),
        out_shape=jax.ShapeDtypeStruct((sp, depth + EDGE, 8 * hd), BF16),
        name="pack",
    )
    packed = packed(row_gain, info, w_x, w_b, w_c, w_z, w_scc, w_scb, w_scx)
    cols = packed.shape[2]
    got = lax.all_to_all(packed, "sp", 0, 0, tiled=True)
    hold = (HOLD * 2 - 1) * parts
    got, *pieces[hold : hold + 2 * parts] = lax.optimization_barrier((got, *pieces[hold : hold + 2 * parts]))
    info = sum(got[:, depth:, k * length : (k + 1) * length].astype(F32) for k in range(3))
    halves = got[:, :depth].reshape(tp, (sp // tp) * depth, cols)
    halves = jnp.broadcast_to(halves, (fs, *halves.shape)).reshape(fs * tp, -1, cols)
    halves = lax.all_to_all(halves, ("fs", "tp"), 0, 0, tiled=True).reshape(fs, tp, sp // tp, depth, cols)

    def head_of(a, dim):
        return lax.dynamic_slice_in_dim(a, here * share * hd, share * hd, dim)

    def group_of(a):
        return lax.dynamic_slice_in_dim(a, (here * share // per_group) * hd, hd, 1)

    taps = jnp.concatenate([head_of(conv_x, 1), group_of(conv_b), group_of(conv_c)], axis=1)
    taps = jnp.pad(taps, ((0, 0), (0, hd)))
    taps_sc = head_of(conv_sc, 1)
    own_gain = head_of(group_gain, 0)[None]
    halves, info, taps, taps_sc, own_gain = lax.optimization_barrier((halves, info, taps, taps_sc, own_gain))

    def w_rows_of(lo, hi):
        some = pieces[lo * parts : hi * parts]
        return pl.pallas_call(
            functools.partial(rows_kernel, parts),
            grid=(1,),
            in_specs=[pl.BlockSpec((depth, half // parts), lambda i: (length // depth, 0))] * len(some),
            out_specs=pl.BlockSpec((hi - lo, depth, half), lambda i: (0, 0, 0)),
            out_shape=jax.ShapeDtypeStruct((hi - lo, depth, half), BF16),
            name="rows",
        )(*some)

    def moved(rows):
        found = [rows]
        for k in range(1, fs):
            found.append(lax.ppermute(rows, "fs", [(i, (i + k) % fs) for i in range(fs)]))
        return found

    cut = 1 + 2 * HOLD
    early = moved(w_rows_of(0, cut))
    late = moved(w_rows_of(cut, sp))

    vmem = pl.BlockSpec(memory_space=pltpu.VMEM)
    smem = pl.BlockSpec(memory_space=pltpu.SMEM)
    project = pl.pallas_call(
        functools.partial(project_kernel, sp, parts, sp // 2 * length, 256),
        in_specs=[smem] * 2 + [vmem] * (len(pieces) + 1),
        out_specs=vmem,
        out_shape=jax.ShapeDtypeStruct((sp, length, cols), BF16),
        scratch_shapes=[pltpu.VMEM((sp * length, half), BF16), pltpu.VMEM((half, cols), BF16)],
        name="project",
    )
    other = project(order, (tp - 1 - side)[None], *pieces, halves)
    arrived = lax.ppermute(other, "tp", swap)
    mine = project(order, side[None], *pieces, halves)

    many = 2
    block = lambda shape: pl.BlockSpec((many, *shape), lambda i: (i,) + (0,) * len(shape))
    whole = lambda a: pl.BlockSpec(a.shape, lambda i: (0,) * a.ndim)
    mixer = pl.pallas_call(
        functools.partial(mixer_kernel, many, taps.shape[0], taps_sc.shape[0]),
        grid=(sp // many,),
        in_specs=[
            block((length, cols)),
            block((length, cols)),
            block((EDGE, length)),
            whole(taps),
            whole(taps_sc),
            whole(own_gain),
        ],
        out_specs=[block((length, 2 * hd)), block((EDGE, length))],
        out_shape=[
            jax.ShapeDtypeStruct((sp, length, 2 * hd), BF16),
            jax.ShapeDtypeStruct((sp, EDGE, length), F32),
        ],
        scratch_shapes=[pltpu.VMEM((EDGE, 6 * hd), F32), pltpu.VMEM((hd, hd), F32)],
        name="mixer",
    )
    ab, squares = mixer(mine, arrived, info, taps, taps_sc, own_gain)

    place = jnp.stack([(fs_here - k) % fs for k in range(fs)])
    w_all = pl.pallas_call(
        assemble_kernel,
        in_specs=[smem] * 2 + [vmem] * (2 * fs),
        out_specs=vmem,
        out_shape=jax.ShapeDtypeStruct((sp * fs * depth, half), BF16),
        name="assemble",
    )(order, place, *early, *late)

    squares = jnp.broadcast_to(squares[:, 0], (per_group, sp, length))
    neighbours = [[g * per_group + k for k in range(per_group)] for g in range(groups)]
    squares = lax.all_to_all(squares, "sp", 0, 0, tiled=True, axis_index_groups=neighbours)
    merged = pl.pallas_call(
        functools.partial(merge_kernel, per_group),
        out_shape=jax.ShapeDtypeStruct((sp, length // 2, 2 * hd), BF16),
        name="merge",
    )(ab, squares)
    merged = lax.all_to_all(merged, "sp", 0, 0, tiled=True)
    partial = pl.pallas_call(
        functools.partial(output_kernel, 512),
        out_shape=jax.ShapeDtypeStruct((length, w_all.shape[0]), BF16),
        scratch_shapes=[pltpu.VMEM((length, half), BF16)],
        name="output",
    )(merged, w_all)
    parts = partial.reshape(tp, length // tp, partial.shape[1])
    parts = lax.all_to_all(parts, "tp", 0, 0, tiled=True)
    return parts.astype(F32).sum(axis=0).astype(BF16)[None]


def solution(mesh):
    return mapped(mesh)


def mapped(mesh):
    return jax.shard_map(
        body,
        mesh=mesh,
        in_specs=(
            P(("grp", "fs"), "sp", "tp"),
            P(),
            P(("sp", "fs"), "tp"),
            P(("sp", "fs"), "tp"),
            P(("sp", "fs"), "tp"),
            P(("sp", "fs"), "tp"),
            P(None, "tp"),
            P(None, None, "tp"),
            P(("sp", "fs"), "tp"),
            P(("sp", "fs"), "tp"),
            P(("sp", "fs"), "tp"),
            P(None, "tp"),
            P(None, "tp"),
            P(None, "tp"),
            P(None, "tp"),
            P("tp"),
            P("tp"),
            P("tp"),
            P(("grp", "fs"), "sp"),
            P(("sp", "fs"), "tp"),
        ),
        out_specs=P(("grp", "fs"), ("sp", "tp"), None),
        check_vma=False,
    )
```

```python
import functools

import jax
import jax.numpy as jnp
from jax import lax
from jax.experimental import pallas as pl
from jax.experimental.pallas import tpu as pltpu
from jax.sharding import PartitionSpec as P


HEAD_DIM = 64
BLOCK = 64
EDGE = 8
HOLD = 4
EPS = 1.0
HIGH = lax.Precision.HIGHEST
F32 = jnp.float32
BF16 = jnp.bfloat16


def silu(v):
    return v / (1.0 + jnp.exp(-v))


def dot(a, b, contract=((1,), (0,))):
    return lax.dot_general(a, b, (contract, ((), ())), preferred_element_type=F32)


def taps_of(extended, taps_ref, count, length):
    first = EDGE - count + 1
    result = extended[first : first + length] * taps_ref[0:1]
    for k in range(1, count):
        result = result + extended[first + k : first + k + length] * taps_ref[k : k + 1]
    return result


def mixer_kernel(
    many, long_taps, short_taps, own_ref, recv_ref, rows_ref, taps_ref, taps_sc_ref, gain_ref, ab_ref, square_ref, tail_ref, state_ref
):
    length = ab_ref.shape[1]
    hd = HEAD_DIM

    @pl.when(pl.program_id(0) == 0)
    def _():
        tail_ref[...] = jnp.zeros_like(tail_ref)
        state_ref[...] = jnp.zeros_like(state_ref)

    lower = lax.broadcasted_iota(jnp.int32, (length, length), 0) >= lax.broadcasted_iota(
        jnp.int32, (length, length), 1
    )
    tail = tail_ref[...]
    state = state_ref[...]
    for k in range(many):
        rows = rows_ref[k]
        cols = rows.T
        step, cum, gate, gate_sc, inverse = (cols[:, i : i + 1] for i in range(5))
        stream = (own_ref[k].astype(F32) + recv_ref[k].astype(F32)) * inverse
        short_in = stream[:, 4 * hd : 5 * hd] * stream[:, 6 * hd : 7 * hd]
        conv = taps_of(jnp.concatenate([tail[:, : 4 * hd], stream[:, : 4 * hd]], axis=0), taps_ref, long_taps, length)
        conv_sc = taps_of(
            jnp.concatenate([tail[:, 4 * hd : 5 * hd], short_in], axis=0), taps_sc_ref, short_taps, length
        )
        tail = jnp.concatenate([stream[length - EDGE :, : 4 * hd], short_in[length - EDGE :], short_in[length - EDGE :]], axis=1)
        conv = silu(conv[:, : 3 * hd])
        x = conv[:, :hd] * step
        b = conv[:, hd : 2 * hd].astype(BF16)
        c = conv[:, 2 * hd : 3 * hd]
        z = stream[:, 3 * hd : 4 * hd]
        scb = stream[:, 5 * hd : 6 * hd]
        scores = dot(c.astype(BF16), b, ((1,), (1,)))
        decay = jnp.where(lower, jnp.exp(jnp.minimum(cum - rows[1:2], 0.0)), 0.0)
        core = dot((scores * decay).astype(BF16), x.astype(BF16))
        core = core + dot((c * jnp.exp(cum)).astype(BF16), state.astype(BF16), ((1,), (1,)))
        last = cum[length - 1 : length]
        fresh = dot((x * jnp.exp(last - cum)).astype(BF16), b, ((0,), (0,)))
        state = state * jnp.exp(last) + fresh
        gated = core * silu(z)
        square_ref[k] = lax.dot_general(
            jnp.ones((EDGE, hd), F32), gated * gated, (((1,), (1,)), ((), ())), precision=HIGH, preferred_element_type=F32
        )
        both = jnp.concatenate([gated * gain_ref[...] * gate, gate_sc * (scb * conv_sc)], axis=1)
        ab_ref[k] = both.astype(BF16)
    tail_ref[...] = tail
    state_ref[...] = state


def merge_kernel(per_group, ab_ref, squares_ref, out_ref):
    hd = HEAD_DIM
    total = squares_ref[0]
    for k in range(1, per_group):
        total = total + squares_ref[k]
    scale = lax.rsqrt(total * (1.0 / (per_group * hd)) + EPS).T
    half = out_ref.shape[1]
    for k in range(out_ref.shape[0]):
        ab = ab_ref[k].astype(F32)
        merged = (ab[:, :hd] * scale[:, k : k + 1] + ab[:, hd:]).astype(BF16)
        out_ref[k] = jnp.concatenate([merged[:half], merged[half:]], axis=1)


def output_kernel(tile, merged_ref, w_ref, out_ref, left_ref):
    count, half, _ = merged_ref.shape
    hd = HEAD_DIM
    for k in range(0, count, 2):
        first, second = merged_ref[k], merged_ref[k + 1]
        lanes = slice(k * hd, (k + 2) * hd)
        left_ref[:half, lanes] = jnp.concatenate([first[:, :hd], second[:, :hd]], axis=1)
        left_ref[half:, lanes] = jnp.concatenate([first[:, hd:], second[:, hd:]], axis=1)
    left = left_ref[...]
    for lo in range(0, out_ref.shape[1], tile):
        out_ref[:, lo : lo + tile] = dot(left, w_ref[lo : lo + tile, :], ((1,), (1,))).astype(BF16)


def rows_kernel(parts, *refs):
    out_ref = refs[-1]
    width = refs[0].shape[1]
    for k in range(out_ref.shape[0]):
        for p in range(parts):
            out_ref[k, :, p * width : (p + 1) * width] = refs[k * parts + p][...]


def pack_kernel(per_group, gain_ref, info_ref, x_ref, b_ref, c_ref, z_ref, scc_ref, scb_ref, scx_ref, out_ref):
    hd = HEAD_DIM
    depth = x_ref.shape[0]
    gain = gain_ref[...]
    scaled = [(ref[...].astype(F32) * gain).astype(BF16) for ref in (x_ref, b_ref, c_ref, z_ref, scc_ref, scb_ref, scx_ref)]
    x, b, c, z, scc, scb, scx = scaled
    for h in range(out_ref.shape[0]):
        g = h // per_group
        own = slice(h * hd, (h + 1) * hd)
        group = slice(g * hd, (g + 1) * hd)
        parts = [x[:, own], b[:, group], c[:, group], z[:, own], scc[:, own], scb[:, own], scx[:, own]]
        parts += [jnp.zeros_like(parts[0])]
        out_ref[h, :depth, :] = jnp.concatenate(parts, axis=1)
        left = info_ref[h]
        split = []
        for _ in range(3):
            part = left.astype(BF16)
            split.append(part)
            left = left - part.astype(F32)
        split.append(jnp.zeros_like(split[0]))
        out_ref[h, depth:, :] = jnp.concatenate(split, axis=1)


def project_kernel(count, parts, rows, tile, order_ref, source_ref, *refs):
    pieces = refs[: count * parts]
    halves_ref, out_ref, tokens_ref, w_ref = refs[count * parts :]
    length, cols = out_ref.shape[1:]
    width = pieces[0].shape[1]
    fs, _, spans, depth, _ = halves_ref.shape
    source = source_ref[0]
    for k in range(count):
        at = pl.multiple_of(order_ref[k] * length, length)
        for p in range(parts):
            tokens_ref[pl.ds(at, length), p * width : (p + 1) * width] = pieces[k * parts + p][:length, :]
    for span in range(spans):
        for f in range(fs):
            lo = (span * fs + f) * depth
            w_ref[lo : lo + depth, :] = halves_ref[f, source, span]

    @pl.loop(0, count * length // rows)
    def _(step):
        left = tokens_ref[pl.ds(pl.multiple_of(step * rows, rows), rows), :]
        for lo in range(0, cols, tile):
            total = dot(left, w_ref[:, lo : lo + tile]).astype(BF16)
            out_ref[pl.ds(step * (rows // length), rows // length), :, lo : lo + tile] = total.reshape(
                rows // length, length, tile
            )


def assemble_kernel(order_ref, place_ref, *refs):
    found, out_ref = refs[:-1], refs[-1]
    count, depth = found[0].shape[:2]
    for k, ref in enumerate(found):
        for j in range(count):
            at = pl.multiple_of((order_ref[j] * len(found) + place_ref[k]) * depth, depth)
            out_ref[pl.ds(at, depth), :] = ref[j]


def ring(x, parts):
    sp, tp = lax.axis_size("sp"), lax.axis_size("tp")
    here, side = lax.axis_index("sp"), lax.axis_index("tp")
    along = [(i * tp + c, (i + 1 - 2 * c) % sp * tp + c) for i in range(sp) for c in range(tp)]
    against = [(b, a) for a, b in along]
    sign = 1 - 2 * side
    width = x.shape[1] // parts
    start = [x[:, p * width : (p + 1) * width] for p in range(parts)]
    ahead, behind = list(start), list(start)
    pieces, order = [start], [here]
    for s in range(1, sp // 2 + 1):
        both = s < sp - sp // 2
        for p in range(parts):
            ahead[p] = lax.ppermute(ahead[p], ("sp", "tp"), along)
            if both:
                behind[p] = lax.ppermute(behind[p], ("sp", "tp"), against)
        pieces.append(list(ahead))
        order.append((here - sign * s) % sp)
        if both:
            pieces.append(list(behind))
            order.append((here + sign * s) % sp)
    return [p for block in pieces for p in block], jnp.stack(order)


def body(
    tokens,
    norm_gain,
    w_z,
    w_x,
    w_b,
    w_c,
    w_dt,
    w_gate,
    w_scb,
    w_scc,
    w_scx,
    conv_x,
    conv_b,
    conv_c,
    conv_sc,
    dt_bias,
    decay_log,
    group_gain,
    span_shift,
    w_out,
):
    sp, fs, tp = (lax.axis_size(a) for a in ("sp", "fs", "tp"))
    here, side, fs_here = (lax.axis_index(a) for a in ("sp", "tp", "fs"))
    own = tokens[0]
    length, half = own.shape
    hd = HEAD_DIM
    heads = dt_bias.shape[0]
    share = heads // sp
    groups = conv_b.shape[1] // hd
    per_group = heads // groups
    depth = w_x.shape[0]

    payload = jnp.concatenate([own, w_out], axis=0)
    parts = 2
    pieces, order = ring(payload, parts)
    swap = [(i, tp - 1 - i) for i in range(tp)]
    partner = lax.ppermute(own, "tp", swap)
    rows = jnp.where(
        side == 0, jnp.concatenate([own, partner], axis=1), jnp.concatenate([partner, own], axis=1)
    ).astype(F32)
    inverse_rms = lax.rsqrt(jnp.mean(rows * rows, axis=1, keepdims=True) + EPS)
    normed = (rows * inverse_rms * norm_gain).astype(BF16)
    narrow = jnp.concatenate([w_dt, w_gate.reshape(w_gate.shape[0], -1)], axis=1)
    small = dot(narrow, normed, ((0,), (1,)))
    shift = jnp.repeat(span_shift[0], BLOCK)
    step = jax.nn.softplus(small[:heads] + dt_bias[:, None] + shift[None, :])
    rate = -jnp.exp(decay_log)[:, None]
    upper = (lax.iota(jnp.int32, length)[:, None] <= lax.iota(jnp.int32, length)[None, :]).astype(F32)
    cum = jnp.dot(step * rate, upper, precision=HIGH)
    gates = jax.nn.sigmoid(small[heads:])
    inverse_rows = jnp.broadcast_to(inverse_rms[:, 0][None, :], (heads, length))
    info = jnp.stack([step, cum, gates[:heads], gates[heads:], inverse_rows], axis=1)
    info = jnp.pad(info, ((0, 0), (0, EDGE - info.shape[1]), (0, 0)))
    row_gain = lax.dynamic_slice_in_dim(norm_gain, (here * fs + fs_here) * depth, depth)[:, None]
    packed = pl.pallas_call(
        functools.partial(pack_kernel, per_group),
        out_shape=jax.ShapeDtypeStruct((sp, depth + EDGE, 8 * hd), BF16),
        name="pack",
    )
    packed = packed(row_gain, info, w_x, w_b, w_c, w_z, w_scc, w_scb, w_scx)
    cols = packed.shape[2]
    got = lax.all_to_all(packed, "sp", 0, 0, tiled=True)
    hold = (HOLD * 2 - 1) * parts
    got, *pieces[hold : hold + 2 * parts] = lax.optimization_barrier((got, *pieces[hold : hold + 2 * parts]))
    info = sum(got[:, depth:, k * length : (k + 1) * length].astype(F32) for k in range(3))
    halves = got[:, :depth].reshape(tp, (sp // tp) * depth, cols)
    halves = jnp.broadcast_to(halves, (fs, *halves.shape)).reshape(fs * tp, -1, cols)
    halves = lax.all_to_all(halves, ("fs", "tp"), 0, 0, tiled=True).reshape(fs, tp, sp // tp, depth, cols)

    def head_of(a, dim):
        return lax.dynamic_slice_in_dim(a, here * share * hd, share * hd, dim)

    def group_of(a):
        return lax.dynamic_slice_in_dim(a, (here * share // per_group) * hd, hd, 1)

    taps = jnp.concatenate([head_of(conv_x, 1), group_of(conv_b), group_of(conv_c)], axis=1)
    taps = jnp.pad(taps, ((0, 0), (0, hd)))
    taps_sc = head_of(conv_sc, 1)
    own_gain = head_of(group_gain, 0)[None]
    halves, info, taps, taps_sc, own_gain = lax.optimization_barrier((halves, info, taps, taps_sc, own_gain))

    def w_rows_of(lo, hi):
        some = pieces[lo * parts : hi * parts]
        return pl.pallas_call(
            functools.partial(rows_kernel, parts),
            grid=(1,),
            in_specs=[pl.BlockSpec((depth, half // parts), lambda i: (length // depth, 0))] * len(some),
            out_specs=pl.BlockSpec((hi - lo, depth, half), lambda i: (0, 0, 0)),
            out_shape=jax.ShapeDtypeStruct((hi - lo, depth, half), BF16),
            name="rows",
        )(*some)

    def moved(rows):
        found = [rows]
        for k in range(1, fs):
            found.append(lax.ppermute(rows, "fs", [(i, (i + k) % fs) for i in range(fs)]))
        return found

    found = moved(w_rows_of(0, sp))

    vmem = pl.BlockSpec(memory_space=pltpu.VMEM)
    smem = pl.BlockSpec(memory_space=pltpu.SMEM)
    project = pl.pallas_call(
        functools.partial(project_kernel, sp, parts, sp // 2 * length, 256),
        in_specs=[smem] * 2 + [vmem] * (len(pieces) + 1),
        out_specs=vmem,
        out_shape=jax.ShapeDtypeStruct((sp, length, cols), BF16),
        scratch_shapes=[pltpu.VMEM((sp * length, half), BF16), pltpu.VMEM((half, cols), BF16)],
        name="project",
    )
    other = project(order, (tp - 1 - side)[None], *pieces, halves)
    arrived = lax.ppermute(other, "tp", swap)
    mine = project(order, side[None], *pieces, halves)

    many = 2
    block = lambda shape: pl.BlockSpec((many, *shape), lambda i: (i,) + (0,) * len(shape))
    whole = lambda a: pl.BlockSpec(a.shape, lambda i: (0,) * a.ndim)
    mixer = pl.pallas_call(
        functools.partial(mixer_kernel, many, taps.shape[0], taps_sc.shape[0]),
        grid=(sp // many,),
        in_specs=[
            block((length, cols)),
            block((length, cols)),
            block((EDGE, length)),
            whole(taps),
            whole(taps_sc),
            whole(own_gain),
        ],
        out_specs=[block((length, 2 * hd)), block((EDGE, length))],
        out_shape=[
            jax.ShapeDtypeStruct((sp, length, 2 * hd), BF16),
            jax.ShapeDtypeStruct((sp, EDGE, length), F32),
        ],
        scratch_shapes=[pltpu.VMEM((EDGE, 6 * hd), F32), pltpu.VMEM((hd, hd), F32)],
        name="mixer",
    )
    ab, squares = mixer(mine, arrived, info, taps, taps_sc, own_gain)

    place = jnp.stack([(fs_here - k) % fs for k in range(fs)])
    w_all = pl.pallas_call(
        assemble_kernel,
        in_specs=[smem] * 2 + [vmem] * fs,
        out_specs=vmem,
        out_shape=jax.ShapeDtypeStruct((sp * fs * depth, half), BF16),
        name="assemble",
    )(order, place, *found)

    squares = jnp.broadcast_to(squares[:, 0], (per_group, sp, length))
    neighbours = [[g * per_group + k for k in range(per_group)] for g in range(groups)]
    squares = lax.all_to_all(squares, "sp", 0, 0, tiled=True, axis_index_groups=neighbours)
    merged = pl.pallas_call(
        functools.partial(merge_kernel, per_group),
        out_shape=jax.ShapeDtypeStruct((sp, length // 2, 2 * hd), BF16),
        name="merge",
    )(ab, squares)
    merged = lax.all_to_all(merged, "sp", 0, 0, tiled=True)
    partial = pl.pallas_call(
        functools.partial(output_kernel, 512),
        out_shape=jax.ShapeDtypeStruct((length, w_all.shape[0]), BF16),
        scratch_shapes=[pltpu.VMEM((length, half), BF16)],
        name="output",
    )(merged, w_all)
    parts = partial.reshape(tp, length // tp, partial.shape[1])
    parts = lax.all_to_all(parts, "tp", 0, 0, tiled=True)
    return parts.astype(F32).sum(axis=0).astype(BF16)[None]


def solution(mesh):
    return mapped(mesh)


def mapped(mesh):
    return jax.shard_map(
        body,
        mesh=mesh,
        in_specs=(
            P(("grp", "fs"), "sp", "tp"),
            P(),
            P(("sp", "fs"), "tp"),
            P(("sp", "fs"), "tp"),
            P(("sp", "fs"), "tp"),
            P(("sp", "fs"), "tp"),
            P(None, "tp"),
            P(None, None, "tp"),
            P(("sp", "fs"), "tp"),
            P(("sp", "fs"), "tp"),
            P(("sp", "fs"), "tp"),
            P(None, "tp"),
            P(None, "tp"),
            P(None, "tp"),
            P(None, "tp"),
            P("tp"),
            P("tp"),
            P("tp"),
            P(("grp", "fs"), "sp"),
            P(("sp", "fs"), "tp"),
        ),
        out_specs=P(("grp", "fs"), ("sp", "tp"), None),
        check_vma=False,
    )
```

```python
import functools

import jax
import jax.numpy as jnp
from jax import lax
from jax.experimental import pallas as pl
from jax.experimental.pallas import tpu as pltpu
from jax.sharding import PartitionSpec as P


HEAD_DIM = 64
BLOCK = 64
EDGE = 8
LANES = 128
HOLD = 4
EPS = 1.0
HIGH = lax.Precision.HIGHEST
F32 = jnp.float32
BF16 = jnp.bfloat16


def silu(v):
    return v / (1.0 + jnp.exp(-v))


def dot(a, b, contract=((1,), (0,))):
    return lax.dot_general(a, b, (contract, ((), ())), preferred_element_type=F32)


def taps_of(extended, taps_ref, count, length):
    first = EDGE - count + 1
    result = extended[first : first + length] * taps_ref[0:1]
    for k in range(1, count):
        result = result + extended[first + k : first + k + length] * taps_ref[k : k + 1]
    return result


def mixer_kernel(
    many, long_taps, short_taps, own_ref, recv_ref, rows_ref, taps_ref, taps_sc_ref, gain_ref, ab_ref, tail_ref, state_ref
):
    length = ab_ref.shape[1] - EDGE
    hd = HEAD_DIM

    @pl.when(pl.program_id(0) == 0)
    def _():
        tail_ref[...] = jnp.zeros_like(tail_ref)
        state_ref[...] = jnp.zeros_like(state_ref)

    lower = lax.broadcasted_iota(jnp.int32, (length, length), 0) >= lax.broadcasted_iota(
        jnp.int32, (length, length), 1
    )
    tail = tail_ref[...]
    state = state_ref[...]
    for k in range(many):
        rows = rows_ref[k]
        cols = rows.T
        step, cum, gate, gate_sc, inverse = (cols[:, i : i + 1] for i in range(5))
        stream = (own_ref[k].astype(F32) + recv_ref[k].astype(F32)) * inverse
        short_in = stream[:, 4 * hd : 5 * hd] * stream[:, 6 * hd : 7 * hd]
        conv = taps_of(jnp.concatenate([tail[:, : 4 * hd], stream[:, : 4 * hd]], axis=0), taps_ref, long_taps, length)
        conv_sc = taps_of(
            jnp.concatenate([tail[:, 4 * hd : 5 * hd], short_in], axis=0), taps_sc_ref, short_taps, length
        )
        tail = jnp.concatenate([stream[length - EDGE :, : 4 * hd], short_in[length - EDGE :], short_in[length - EDGE :]], axis=1)
        conv = silu(conv[:, : 3 * hd])
        x = conv[:, :hd] * step
        b = conv[:, hd : 2 * hd].astype(BF16)
        c = conv[:, 2 * hd : 3 * hd]
        z = stream[:, 3 * hd : 4 * hd]
        scb = stream[:, 5 * hd : 6 * hd]
        scores = dot(c.astype(BF16), b, ((1,), (1,)))
        decay = jnp.where(lower, jnp.exp(jnp.minimum(cum - rows[1:2], 0.0)), 0.0)
        core = dot((scores * decay).astype(BF16), x.astype(BF16))
        core = core + dot((c * jnp.exp(cum)).astype(BF16), state.astype(BF16), ((1,), (1,)))
        last = cum[length - 1 : length]
        fresh = dot((x * jnp.exp(last - cum)).astype(BF16), b, ((0,), (0,)))
        state = state * jnp.exp(last) + fresh
        gated = core * silu(z)
        squares = lax.dot_general(
            jnp.ones((EDGE, hd), F32), gated * gated, (((1,), (1,)), ((), ())), precision=HIGH, preferred_element_type=F32
        )
        coarse = squares.astype(BF16)
        fine = (squares - coarse.astype(F32)).astype(BF16)
        which = lax.broadcasted_iota(jnp.int32, squares.shape, 0)
        packed = jnp.where(which == 0, coarse.astype(F32), jnp.where(which == 1, fine.astype(F32), 0.0))
        both = jnp.concatenate([gated * gain_ref[...] * gate, gate_sc * (scb * conv_sc)], axis=1)
        ab_ref[k] = jnp.concatenate([both, packed], axis=0).astype(BF16)
    tail_ref[...] = tail
    state_ref[...] = state


def merge_kernel(per_group, ab_ref, out_ref):
    count, full = ab_ref.shape[0], ab_ref.shape[1]
    length = full - EDGE
    hd = HEAD_DIM
    ones = jnp.ones((per_group * EDGE, LANES), BF16)
    for g in range(count // per_group):
        squares = jnp.concatenate([ab_ref[g * per_group + k, length:, :] for k in range(per_group)], axis=0)
        mean = dot(squares, ones, ((0,), (0,))) * (1.0 / (per_group * hd))
        scale = lax.rsqrt(mean + EPS)[:, :hd]
        for k in range(0, per_group, 2):
            pair = []
            for j in range(2):
                ab = ab_ref[g * per_group + k + j, :length, :].astype(F32)
                pair.append(ab[:, :hd] * scale + ab[:, hd:])
            lo = (g * per_group + k) * hd
            out_ref[:, lo : lo + 2 * hd] = jnp.concatenate(pair, axis=1).astype(out_ref.dtype)


def pack_kernel(per_group, x_ref, b_ref, c_ref, z_ref, scc_ref, scb_ref, scx_ref, out_ref):
    hd = HEAD_DIM
    for h in range(out_ref.shape[0]):
        g = h // per_group
        own = slice(h * hd, (h + 1) * hd)
        group = slice(g * hd, (g + 1) * hd)
        parts = [x_ref[:, own], b_ref[:, group], c_ref[:, group], z_ref[:, own]]
        parts += [scc_ref[:, own], scb_ref[:, own], scx_ref[:, own]]
        parts += [jnp.zeros_like(parts[0])]
        out_ref[h] = jnp.concatenate(parts, axis=1)


def project_kernel(count, parts, batch, tile, order_ref, *refs):
    pieces = refs[: count * parts]
    w_ref, mine_ref, other_ref, rows_ref = refs[count * parts :]
    length, cols = mine_ref.shape[1:]
    extra = rows_ref.shape[1]
    width = pieces[0].shape[1]
    for g in range(0, count, batch):
        group = pieces[g * parts : (g + batch) * parts]
        places = [order_ref[g + j] for j in range(batch)]

        @pl.loop(0, cols // tile)
        def _(step):
            at = pl.multiple_of(step * tile, tile)
            for side, out_ref in enumerate((mine_ref, other_ref)):
                column = pl.ds(pl.multiple_of(side * cols + step * tile, tile), tile)
                total = 0.0
                for p in range(parts):
                    left = jnp.concatenate([group[j * parts + p][:length, :] for j in range(batch)], axis=0)
                    total = total + dot(left, w_ref[p * width : (p + 1) * width, column])
                for j in range(batch):
                    out_ref[places[j], :, pl.ds(at, tile)] = total[j * length : (j + 1) * length].astype(BF16)

        for j in range(batch):
            for p in range(parts):
                rows_ref[places[j], :, p * width : (p + 1) * width] = group[j * parts + p][length : length + extra, :]


def ring(x, parts):
    sp, tp = lax.axis_size("sp"), lax.axis_size("tp")
    here, side = lax.axis_index("sp"), lax.axis_index("tp")
    along = [(i * tp + c, (i + 1 - 2 * c) % sp * tp + c) for i in range(sp) for c in range(tp)]
    against = [(b, a) for a, b in along]
    sign = 1 - 2 * side
    width = x.shape[1] // parts
    start = [x[:, p * width : (p + 1) * width] for p in range(parts)]
    ahead, behind = list(start), list(start)
    pieces, order = [start], [here]
    for s in range(1, sp // 2 + 1):
        both = s < sp - sp // 2
        ahead = [lax.ppermute(a, ("sp", "tp"), along) for a in ahead]
        if both:
            behind = [lax.ppermute(a, ("sp", "tp"), against) for a in behind]
        if both:
            for p in range(parts):
                ahead[p], behind[p] = lax.optimization_barrier((ahead[p], behind[p]))
        pieces.append(list(ahead))
        order.append((here - sign * s) % sp)
        if both:
            pieces.append(list(behind))
            order.append((here + sign * s) % sp)
    return [p for block in pieces for p in block], jnp.stack(order)


def body(
    tokens,
    norm_gain,
    w_z,
    w_x,
    w_b,
    w_c,
    w_dt,
    w_gate,
    w_scb,
    w_scc,
    w_scx,
    conv_x,
    conv_b,
    conv_c,
    conv_sc,
    dt_bias,
    decay_log,
    group_gain,
    span_shift,
    w_out,
):
    sp, fs, tp = (lax.axis_size(a) for a in ("sp", "fs", "tp"))
    here, side = lax.axis_index("sp"), lax.axis_index("tp")
    own = tokens[0]
    length, half = own.shape
    hd = HEAD_DIM
    heads = dt_bias.shape[0]
    share = heads // sp
    groups = conv_b.shape[1] // hd
    per_group = heads // groups
    depth = depth_own = w_x.shape[0]

    pack = pl.pallas_call(
        functools.partial(pack_kernel, per_group),
        out_shape=jax.ShapeDtypeStruct((sp, depth_own, 8 * hd), BF16),
        name="pack",
    )
    packed = pack(w_x, w_b, w_c, w_z, w_scc, w_scb, w_scx)
    cols = packed.shape[2]
    got = lax.all_to_all(packed, "sp", 0, 0, tiled=True)

    payload = jnp.concatenate([own, w_out], axis=0)
    parts = 2
    pieces, order = ring(payload, parts)
    hold = (HOLD * 2 - 1) * parts

    got, *pieces[hold : hold + parts] = lax.optimization_barrier((got, *pieces[hold : hold + parts]))
    halves = got.reshape(tp, (sp // tp) * depth, cols)
    halves = jnp.broadcast_to(halves, (fs, *halves.shape)).reshape(fs * tp, -1, cols)
    halves = lax.all_to_all(halves, ("fs", "tp"), 0, 0, tiled=True)
    weights = halves.reshape(fs, tp, sp // tp, depth, cols).transpose(1, 2, 0, 3, 4).reshape(tp, half, cols)
    gain = lax.dynamic_slice_in_dim(norm_gain, side * half, half)
    weights = (weights.astype(F32) * gain[:, None]).astype(BF16)
    w_mine = lax.dynamic_index_in_dim(weights, side, 0, keepdims=False)
    w_other = lax.dynamic_index_in_dim(weights, (tp - 1) - side, 0, keepdims=False)

    swap = [(i, tp - 1 - i) for i in range(tp)]
    partner = lax.ppermute(own, "tp", swap)
    rows = jnp.where(
        side == 0, jnp.concatenate([own, partner], axis=1), jnp.concatenate([partner, own], axis=1)
    ).astype(F32)
    inverse_rms = lax.rsqrt(jnp.mean(rows * rows, axis=1, keepdims=True) + EPS)
    normed = (rows * inverse_rms * norm_gain).astype(BF16)
    narrow = jnp.concatenate([w_dt, w_gate.reshape(w_gate.shape[0], -1)], axis=1)
    small = dot(narrow, normed, ((0,), (1,)))
    shift = jnp.repeat(span_shift[0], BLOCK)
    step = jax.nn.softplus(small[:heads] + dt_bias[:, None] + shift[None, :])
    rate = -jnp.exp(decay_log)[:, None]
    upper = (lax.iota(jnp.int32, length)[:, None] <= lax.iota(jnp.int32, length)[None, :]).astype(F32)
    cum = jnp.dot(step * rate, upper, precision=HIGH)
    gates = jax.nn.sigmoid(small[heads:])
    inverse_rows = jnp.broadcast_to(inverse_rms[:, 0][None, :], (heads, length))
    info = jnp.stack([step, cum, gates[:heads], gates[heads:], inverse_rows], axis=1)
    info = jnp.pad(info, ((0, 0), (0, EDGE - info.shape[1]), (0, 0)))
    info = lax.all_to_all(info, "sp", 0, 0, tiled=True)

    vmem = pl.BlockSpec(memory_space=pltpu.VMEM)
    w_both = jnp.concatenate([w_mine, w_other], axis=1)
    project = pl.pallas_call(
        functools.partial(project_kernel, sp, parts, 4, 256),
        in_specs=[pl.BlockSpec(memory_space=pltpu.SMEM)] + [vmem] * (len(pieces) + 1),
        out_specs=[vmem] * 3,
        out_shape=[
            jax.ShapeDtypeStruct((sp, length, cols), BF16),
            jax.ShapeDtypeStruct((sp, length, cols), BF16),
            jax.ShapeDtypeStruct((sp, depth, half), BF16),
        ],
        name="project",
    )
    mine, other, w_rows = project(order, *pieces, w_both)
    arrived = lax.ppermute(other, "tp", swap)

    def head_of(a, dim):
        return lax.dynamic_slice_in_dim(a, here * share * hd, share * hd, dim)

    def group_of(a):
        return lax.dynamic_slice_in_dim(a, (here * share // per_group) * hd, hd, 1)

    taps = jnp.concatenate([head_of(conv_x, 1), group_of(conv_b), group_of(conv_c)], axis=1)
    taps = jnp.pad(taps, ((0, 0), (0, hd)))
    taps_sc = head_of(conv_sc, 1)
    own_gain = head_of(group_gain, 0)[None]
    many = 2
    block = lambda shape: pl.BlockSpec((many, *shape), lambda i: (i,) + (0,) * len(shape))
    whole = lambda a: pl.BlockSpec(a.shape, lambda i: (0,) * a.ndim)
    mixer = pl.pallas_call(
        functools.partial(mixer_kernel, many, taps.shape[0], taps_sc.shape[0]),
        grid=(sp // many,),
        in_specs=[
            block((length, cols)),
            block((length, cols)),
            block((EDGE, length)),
            whole(taps),
            whole(taps_sc),
            whole(own_gain),
        ],
        out_specs=block((length + EDGE, 2 * hd)),
        out_shape=jax.ShapeDtypeStruct((sp, length + EDGE, 2 * hd), BF16),
        scratch_shapes=[pltpu.VMEM((EDGE, 6 * hd), F32), pltpu.VMEM((hd, hd), F32)],
        name="mixer",
    )
    ab = mixer(mine, arrived, info, taps, taps_sc, own_gain)

    w_rows = w_rows.reshape(-1, half)
    fs_here = lax.axis_index("fs")
    w_parts = [w_rows]
    for k in range(1, fs):
        w_parts.append(lax.ppermute(w_rows, "fs", [(i, (i + k) % fs) for i in range(fs)]))
    w_parts = jnp.stack(w_parts)
    w_all = [lax.dynamic_index_in_dim(w_parts, (fs_here - k) % fs, 0, keepdims=False) for k in range(fs)]
    w_all = jnp.stack([w.reshape(sp, depth, half) for w in w_all], axis=1).reshape(-1, half)
    ab = lax.all_to_all(ab, "sp", 0, 0, tiled=True)
    merged = pl.pallas_call(
        functools.partial(merge_kernel, per_group),
        out_shape=jax.ShapeDtypeStruct((length, sp * hd), BF16),
        name="merge",
    )(ab)
    partial = dot(merged, w_all, ((1,), (1,))).astype(BF16)
    parts = partial.reshape(tp, length // tp, partial.shape[1])
    parts = lax.all_to_all(parts, "tp", 0, 0, tiled=True)
    return parts.astype(F32).sum(axis=0).astype(BF16)[None]


def solution(mesh):
    return mapped(mesh)


def mapped(mesh):
    return jax.shard_map(
        body,
        mesh=mesh,
        in_specs=(
            P(("grp", "fs"), "sp", "tp"),
            P(),
            P(("sp", "fs"), "tp"),
            P(("sp", "fs"), "tp"),
            P(("sp", "fs"), "tp"),
            P(("sp", "fs"), "tp"),
            P(None, "tp"),
            P(None, None, "tp"),
            P(("sp", "fs"), "tp"),
            P(("sp", "fs"), "tp"),
            P(("sp", "fs"), "tp"),
            P(None, "tp"),
            P(None, "tp"),
            P(None, "tp"),
            P(None, "tp"),
            P("tp"),
            P("tp"),
            P("tp"),
            P(("grp", "fs"), "sp"),
            P(("sp", "fs"), "tp"),
        ),
        out_specs=P(("grp", "fs"), ("sp", "tp"), None),
        check_vma=False,
    )
```
